256 devices in a mesh: st: 64 (over z, x, core), tp: 4 (over y).
Axes of the slice: x: 4, y: 4, z: 8, core: 2. Of those that a mesh axis runs over, the one named last changes fastest.
Arguments:
- tokens: bfloat16 [65536, 4096], P('st'), may hold values from -6 to 6
- passage_ids: int32 [1024, 4], P('st'), may hold values from 0 to 191, as said below
- store: bfloat16 [192, 128, 4096], P('st'), may hold values from -6 to 6
- mix_gain: bfloat16 [4096], replicated, may hold values from 0.099609375 to 1.8984375
- w_query: bfloat16 [4096, 512], P(None, 'tp'), may hold values from -0.09375 to 0.09375
- w_key: bfloat16 [4096, 512], P(None, 'tp'), may hold values from -0.09375 to 0.09375
- w_value: bfloat16 [4096, 512], P(None, 'tp'), may hold values from -0.09375 to 0.09375
- w_cross_out: bfloat16 [512, 1024], P('tp'), may hold values from -0.5 to 0.5
- head_scale: float32 [4], replicated, may hold values from 1 to 4
- w_pool_in: bfloat16 [4096, 1024], P(None, 'tp'), may hold values from -0.09375 to 0.09375
- w_pool_mix: bfloat16 [4, 256, 256], replicated, may hold values from -0.375 to 0.375
- pool_scale: bfloat16 [1024], replicated, may hold values from 0.099609375 to 1.8984375
- gate_weight: float32 [1024], replicated, may hold values from -4 to 4
Outputs:
- mixed: bfloat16 [65536, 1024], P('st', 'tp')
The draws below stay inside these ranges and needn't reach their ends.
Inputs may be any that keep to these rules, and one draw needn't show every extreme that they name: `passage_ids`: passage p is held by index p // 3 of st. The 64 ids of one index of st (its aligned blocks of rows) fall on exactly 32 owners, 2 ids on each; one owner receives 2 ids from every index of st.
All inputs are finite; a program needn't handle non-finite values.
Results may differ from the reference program's by a relative error of at most 0.013.
Values may be sent and summed in bfloat16 or wider, within the bound.
A program may use at most 128 MiB of HBM per device.

```python
import math
import jax
import jax.numpy as jnp
from jax import lax

D = 4096
HEADS = 4
HEAD_DIM = 128
POOL_WIDTH = 1024
POOL_GROUPS = 4
GROUP_WIDTH = 256
SEQ_LEN = 128
BLOCK = 64
NPB = 4
P_LEN = 128
PASS_DEV = 3
TOKENS = 65536
BLOCKS = 1024
PASSAGES = 192
REQ_DEV = 64
CAP = 2
N_ST = 64


def draw_passage_ids(key, part):
    hot_owner = jax.random.randint(jax.random.fold_in(key, 7), (), 0, N_ST)
    shifts = jnp.arange(N_ST).astype(jnp.int32)

    def one_device(device):
        device_key = jax.random.fold_in(key, device + 1000)
        priority = jax.random.randint(jax.random.fold_in(device_key, 1), (N_ST,), 0, 1 << 20) * N_ST + shifts
        priority = jnp.where(shifts == N_ST - 1, -3, priority)
        priority = jnp.where(shifts == N_ST // 2, jnp.minimum(priority, -2), priority)
        priority = jnp.where(shifts == (hot_owner - device) % N_ST, jnp.minimum(priority, -1), priority)
        ordering = jnp.argsort(priority, stable=True).astype(jnp.int32)
        owners = (device + ordering[jnp.arange(REQ_DEV) // CAP]) % N_ST
        first_pick = jax.random.randint(jax.random.fold_in(device_key, 2), (REQ_DEV,), 0, PASS_DEV)
        second_pick = jax.random.randint(jax.random.fold_in(device_key, 3), (REQ_DEV,), 0, PASS_DEV)
        chosen = owners * PASS_DEV + jnp.minimum(first_pick, second_pick)
        shuffle = jax.random.permutation(jax.random.fold_in(device_key, 4), REQ_DEV)
        return chosen[shuffle]
    all_ids = jax.vmap(one_device)(jnp.arange(N_ST).astype(jnp.int32))
    return all_ids.reshape(N_ST * REQ_DEV // NPB, NPB).astype(jnp.int32)


def shard_levels(rng, dims, pieces, low, largest):
    def one(axis_at, parts):
        heights = jax.random.uniform(jax.random.fold_in(jax.random.fold_in(rng, 6), axis_at), (parts,), jnp.float32, low / len(pieces), largest / len(pieces))
        return jnp.repeat(jnp.exp(heights), dims[axis_at] // parts).reshape((-1,) + (1,) * (len(dims) - axis_at - 1))

    level = one(*pieces[0])
    for cut in pieces[1:]:
        level = level * one(*cut)
    return level


def centred(rng, dims, spread, reach, split=(), kind=jnp.bfloat16):
    drawn = spread * jax.random.normal(rng, dims, jnp.float32)
    if split:
        drawn = drawn * shard_levels(rng, dims, split, -0.22, 0.18)
    return jnp.clip(drawn, -reach, reach).astype(kind)


def setup_inputs(seed: int = 0) -> dict:
    keys = jax.random.split(jax.random.key(seed), 14)
    return {
        "tokens": centred(keys[0], (TOKENS, D), 1.0, 6.0, ((0, 64),)),
        "passage_ids": draw_passage_ids(jax.random.fold_in(keys[13], 71), 0),
        "store": centred(keys[2], (PASSAGES, P_LEN, D), 1.0, 6.0, ((0, 64),)),
        "mix_gain": jnp.clip(1.0 + 0.18 * jax.random.normal(keys[3], (D,), jnp.float32), 0.099609375, 1.8984375).astype(jnp.bfloat16),
        "w_query": centred(keys[4], (D, HEADS * HEAD_DIM), D ** -0.5, 0.09375, ((1, 4),)),
        "w_key": centred(keys[5], (D, HEADS * HEAD_DIM), D ** -0.5, 0.09375, ((1, 4),)),
        "w_value": centred(keys[6], (D, HEADS * HEAD_DIM), D ** -0.5, 0.09375, ((1, 4),)),
        "w_cross_out": centred(keys[7], (HEADS * HEAD_DIM, POOL_WIDTH), HEAD_DIM ** -0.5, 0.5, ((0, 4),)),
        "head_scale": jnp.clip(jnp.exp(jax.random.uniform(keys[8], (HEADS,), jnp.float32, math.log(1.0), math.log(4.0))), 1.0, 4.0),
        "w_pool_in": centred(keys[9], (D, POOL_WIDTH), D ** -0.5, 0.09375, ((1, 4),)),
        "w_pool_mix": centred(keys[10], (POOL_GROUPS, GROUP_WIDTH, GROUP_WIDTH), GROUP_WIDTH ** -0.5, 0.375),
        "pool_scale": jnp.clip(1.0 + 0.18 * jax.random.normal(keys[11], (POOL_WIDTH,), jnp.float32), 0.099609375, 1.8984375).astype(jnp.bfloat16),
        "gate_weight": centred(keys[12], (POOL_WIDTH,), 1.0, 4.0, (), jnp.float32),
    }


EPSILON = 1e-06

def head_normalize(values):
    return values * lax.rsqrt(lax.optimization_barrier(jnp.mean(values * values, axis=-1, keepdims=True)) + EPSILON)

def normalize_rows(tokens, mix_gain):
    floats = tokens.astype(jnp.float32)
    scaled = floats * lax.rsqrt(lax.optimization_barrier(jnp.mean(floats * floats, axis=-1, keepdims=True)) + EPSILON)
    return (scaled * mix_gain.astype(jnp.float32)).astype(jnp.bfloat16)

def pool_residual(pooled_in, channel_ids):
    row_count, chan_width = pooled_in.shape
    sequences = pooled_in.astype(jnp.float32).reshape(row_count // SEQ_LEN, SEQ_LEN, chan_width)
    running = jnp.cumsum(sequences, axis=1)
    padded = jnp.concatenate([jnp.zeros((sequences.shape[0], 16, chan_width), jnp.float32), running], axis=1)
    upper_sum = padded[:, 16:]
    position = jnp.arange(SEQ_LEN).astype(jnp.int32)[None, :, None]
    result = jnp.zeros_like(sequences)
    for section_index in range(4):
        window = 2 << section_index
        lower_sum = padded[:, 16 - window:16 - window + SEQ_LEN]
        counted = jnp.minimum(position + 1, window).astype(jnp.float32)
        average = (upper_sum - lower_sum) / counted
        chosen = (channel_ids // GROUP_WIDTH == section_index)[None, None, :]
        result = jnp.where(chosen, average - sequences, result)
    return result.reshape(row_count, chan_width).astype(jnp.bfloat16)

def reference(tokens, passage_ids, store, mix_gain, w_query, w_key, w_value, w_cross_out, head_scale, w_pool_in, w_pool_mix, pool_scale, gate_weight):
    normed = normalize_rows(tokens, mix_gain)
    pooled_in = jnp.dot(normed, w_pool_in, preferred_element_type=jnp.float32).astype(jnp.bfloat16)
    residual = pool_residual(pooled_in, jnp.arange(POOL_WIDTH).astype(jnp.int32))
    grouped = residual.astype(jnp.float32).reshape(TOKENS, POOL_GROUPS, GROUP_WIDTH)
    pool_out = jnp.einsum('tgc,gce->tge', grouped, w_pool_mix.astype(jnp.float32)).reshape(TOKENS, POOL_WIDTH)
    pool_out = pool_out * pool_scale.astype(jnp.float32)
    queries = head_normalize(jnp.dot(normed, w_query, preferred_element_type=jnp.float32).reshape(TOKENS, HEADS, HEAD_DIM)).astype(jnp.bfloat16)
    flat_store = store.reshape(PASSAGES * P_LEN, D)
    passage_keys = head_normalize(jnp.dot(flat_store, w_key, preferred_element_type=jnp.float32).reshape(PASSAGES, P_LEN, HEADS, HEAD_DIM)).astype(jnp.bfloat16)
    passage_values = jnp.dot(flat_store, w_value, preferred_element_type=jnp.float32).astype(jnp.bfloat16).reshape(PASSAGES, P_LEN, HEADS, HEAD_DIM)
    scales = head_scale.astype(jnp.float32) / math.sqrt(HEAD_DIM)

    def one_block(inputs):
        block_queries, block_ids = inputs
        block_keys = passage_keys[block_ids].astype(jnp.float32)
        block_values = passage_values[block_ids].astype(jnp.float32)
        scores = jnp.einsum('qhd,jkhd->hqjk', block_queries.astype(jnp.float32), block_keys) * scales[:, None, None, None]
        weights = jnp.exp(scores)
        totals = lax.optimization_barrier(jnp.sum(weights, axis=(2, 3)))
        rounded = lax.optimization_barrier(weights.astype(jnp.bfloat16))
        partial_out = jnp.einsum('hqjk,jkhd->jqhd', rounded.astype(jnp.float32), block_values)
        partial_out = lax.optimization_barrier(partial_out.astype(jnp.bfloat16))
        summed = lax.optimization_barrier(jnp.sum(partial_out.astype(jnp.float32), axis=0))
        return (summed / jnp.transpose(totals)[:, :, None]).astype(jnp.bfloat16)
    attended = lax.map(one_block, (queries.reshape(BLOCKS, BLOCK, HEADS, HEAD_DIM), passage_ids))
    attended = attended.reshape(TOKENS, HEADS, HEAD_DIM)
    cross_sum = jnp.zeros((TOKENS, POOL_WIDTH), jnp.float32)
    for head_index in range(HEADS):
        rows_of_head = w_cross_out[head_index * HEAD_DIM:(head_index + 1) * HEAD_DIM]
        cross_term = jnp.dot(attended[:, head_index], rows_of_head, preferred_element_type=jnp.float32)
        cross_term = lax.optimization_barrier(cross_term.astype(jnp.bfloat16))
        cross_sum = cross_sum + cross_term.astype(jnp.float32)
    gate_value = jax.nn.sigmoid(pooled_in.astype(jnp.float32) * gate_weight.astype(jnp.float32))
    return (pool_out + gate_value * cross_sum).astype(jnp.bfloat16)
```

```python
import functools
import math

import jax
import jax.numpy as jnp
from jax import lax
from jax.experimental import pallas as pl
from jax.experimental.pallas import tpu as pltpu
from jax.sharding import PartitionSpec as P

MESH = pl.DeviceIdType.MESH
BF = jnp.bfloat16
F32 = jnp.float32

EPSILON = 1e-06
NZ, NX, NC, NY = 8, 4, 2, 4
D = 4096
HD = 128
GW = 256
ROWS = 1024
BLOCK = 64
NPB = 4
NBLK = 16
PLEN = 128
OWN = 3
SEQ = 128
SLOTS = NZ * NC * OWN
TCHUNK = 256
QTR = 256


def kernel(
    tok_h, ids_h, store_h, gain_h, wq_h, wk_h, wv_h, wc_h, hs_s, wp_h, wm_h, ps_h, gw_h,
    out_h,
    tok_v, store_v, wkv_v, wq_v, wp_v, wm_v, gain_v, ps_v, gw_v,
    kt_v, v_v, qg_v, idv, ids_s, wc_v,
    pooled_v, pool_v, gate_v, e_v, part_v, rly_v, sum_v, rrecv_v, tot_v, totg_v, att_v, out_v,
    lsem, tsem, osem,
    zs, zr, cs, cr, qs, qr, ids_ss, ids_rs, wcs, wcr, ts, tr, rs, rr, ys, yr,
):
    s = lax.axis_index("st")
    y = lax.axis_index("tp")
    c = lax.rem(s, NC)
    x = lax.rem(lax.div(s, NC), NX)
    z = lax.div(s, NC * NX)

    def dev(dz=0, dx=0, dy=0, other=False):
        cc = 1 - c if other else c
        zz = lax.rem(z + dz + NZ, NZ)
        xx = lax.rem(x + dx + NX, NX)
        yy = lax.rem(y + dy + NY, NY)
        return (zz * (NX * NC) + xx * NC + cc, yy)

    def remote(src, dst, ssem, rsem, to):
        return pltpu.make_async_remote_copy(
            src_ref=src, dst_ref=dst, send_sem=ssem, recv_sem=rsem,
            device_id=to, device_id_type=MESH,
        )

    barrier = pltpu.get_barrier_semaphore()
    partners = [
        dev(dz=1), dev(dz=-1), dev(dx=1), dev(dx=-1), dev(dx=2),
        dev(dy=1), dev(dy=-1), dev(dy=2), dev(other=True),
    ]
    for to in partners:
        pl.semaphore_signal(barrier, inc=1, device_id=to, device_id_type=MESH)

    def local(src, dst, sem):
        copy = pltpu.make_async_copy(src, dst, sem)
        copy.start()
        return copy

    kv_loads = [
        local(wk_h, wkv_v.at[:, pl.ds(0, HD)], lsem.at[0]),
        local(wv_h, wkv_v.at[:, pl.ds(HD, HD)], lsem.at[1]),
        local(store_h, store_v, lsem.at[2]),
    ]
    gain_load = local(gain_h, gain_v, lsem.at[3])
    wq_load = local(wq_h, wq_v, lsem.at[4])
    tok_loads = [
        local(
            tok_h.at[pl.ds(i * TCHUNK, TCHUNK)], tok_v.at[pl.ds(i * TCHUNK, TCHUNK)], tsem.at[i]
        )
        for i in range(ROWS // TCHUNK)
    ]
    wp_load = local(wp_h, wp_v, lsem.at[5])
    pool_loads = [
        local(wm_h.at[y], wm_v, lsem.at[6]),
        local(ps_h, ps_v, lsem.at[7]),
        local(gw_h, gw_v, lsem.at[8]),
    ]
    ids_own = local(ids_h, idv.at[0], lsem.at[9])
    wc_own = local(
        wc_h.at[:, pl.ds(pl.multiple_of(y * GW, GW), GW)], wc_v.at[y], lsem.at[10]
    )

    pl.semaphore_wait(barrier, len(partners))

    sends = []

    for r in (1, 2, 3):
        cp = remote(ids_h, idv.at[NX - r], ids_ss.at[r], ids_rs.at[NX - r], dev(dx=r))
        cp.start()
        sends.append(cp)
    for r in (1, 2, 3):
        column = pl.multiple_of(lax.rem(y + r, NY) * GW, GW)
        cp = remote(
            wc_h.at[:, pl.ds(column, GW)], wc_v.at[y], wcs.at[r], wcr.at[NY - r], dev(dy=r)
        )
        cp.start()
        sends.append(cp)

    for load in kv_loads:
        load.wait()
    kv = jnp.dot(store_v[...].reshape(OWN * PLEN, D), wkv_v[...], preferred_element_type=F32)
    keys = kv[:, :HD]
    keys = keys * lax.rsqrt(jnp.mean(keys * keys, axis=-1, keepdims=True) + EPSILON)
    own_slot = (z * NC + c) * OWN
    for i in range(OWN):
        rows = slice(i * PLEN, (i + 1) * PLEN)
        kt_v[own_slot + i] = jnp.transpose(keys[rows]).astype(BF)
        v_v[own_slot + i] = kv[rows, HD:].astype(BF)

    bufs = (kt_v, v_v)

    def group(kind, origin, core):
        return bufs[kind].at[pl.ds((origin * NC + core) * OWN, OWN)]

    def z_copy(d, kind, k, to_next):
        sign = 1 if d == 0 else -1
        back = k if to_next else k + 1
        origin = lax.rem(z - sign * back + NZ, NZ)
        block = group(kind, origin, c)
        i = d * 8 + kind * 4 + k
        return remote(block, block, zs.at[i], zr.at[i], dev(dz=sign))

    def z_send(d, kind, k):
        cp = z_copy(d, kind, k, True)
        cp.start()
        sends.append(cp)

    def core_send(kind, o):
        block = group(kind, lax.rem(z + o, NZ), c)
        i = kind * NZ + o
        cp = remote(block, block, cs.at[i], cr.at[i], dev(other=True))
        cp.start()
        sends.append(cp)

    def core_wait(kind, o):
        block = group(kind, lax.rem(z + o, NZ), 1 - c)
        i = kind * NZ + o
        remote(block, block, cs.at[i], cr.at[i], dev(other=True)).wait_recv()

    def z_advance(d, kind, k):
        z_copy(d, kind, k, False).wait_recv()
        if k < 2 or (k == 2 and kind == d):
            z_send(d, kind, k + 1)
        back = k + 1
        core_send(kind, back if d == 1 else NZ - back)

    for kind in (0, 1):
        for d in (0, 1):
            z_send(d, kind, 0)
    for kind in (0, 1):
        core_send(kind, 0)

    gain_load.wait()
    wq_load.wait()
    gain = gain_v[...]

    def q_copy(d, m, sending):
        sign = 1 if d == 0 else -1
        if m < 2:
            half, back = m, 0
        else:
            half, back = d, 1
        origin = back if sending else back + 1
        row = (origin if d == 1 else NX - origin) % NX
        at = qg_v.at[row, pl.ds(half * (ROWS // 2), ROWS // 2)]
        back_there = back + 1
        row_there = (back_there if d == 1 else NX - back_there) % NX
        to = qg_v.at[row_there, pl.ds(half * (ROWS // 2), ROWS // 2)] if sending else at
        i = d * 3 + m
        return remote(at, to, qs.at[i], qr.at[i], dev(dx=sign))

    def q_send(d, m):
        cp = q_copy(d, m, True)
        cp.start()
        sends.append(cp)

    scales = []

    def query_chunk(i):
        tok_loads[i].wait()
        t = tok_v[pl.ds(i * TCHUNK, TCHUNK), :]
        tf = t.astype(F32)
        scale = lax.rsqrt(jnp.mean(tf * tf, axis=-1, keepdims=True) + EPSILON)
        scales.append(scale)
        tg = t * gain
        tok_v[pl.ds(i * TCHUNK, TCHUNK), :] = tg
        q = jnp.dot(tg, wq_v[...], preferred_element_type=F32) * scale
        q = q * lax.rsqrt(jnp.mean(q * q, axis=-1, keepdims=True) + EPSILON)
        qg_v[0, pl.ds(i * TCHUNK, TCHUNK), :] = q.astype(BF)

    per_half = ROWS // 2 // TCHUNK
    for half in (0, 1):
        for i in range(per_half):
            query_chunk(half * per_half + i)
        for d in (0, 1):
            q_send(d, half)

    for kind in (0, 1):
        for d in (0, 1):
            z_advance(d, kind, 0)

    wp_load.wait()
    for i in range(ROWS // TCHUNK):
        tg = tok_v[pl.ds(i * TCHUNK, TCHUNK), :]
        pooled = jnp.dot(tg, wp_v[...], preferred_element_type=F32) * scales[i]
        pooled_v[pl.ds(i * TCHUNK, TCHUNK), :] = pooled.astype(BF)

    for d in (0, 1):
        z_advance(d, 0, 1)

    for d in (0, 1):
        q_copy(d, d, False).wait_recv()
        q_send(d, 2)

    for load in pool_loads:
        load.wait()
    window = lax.shift_left(jnp.int32(2), y.astype(jnp.int32))
    row_id = lax.broadcasted_iota(jnp.int32, (SEQ, SEQ), 0)
    col_id = lax.broadcasted_iota(jnp.int32, (SEQ, SEQ), 1)
    band = jnp.where((col_id <= row_id) & (col_id > row_id - window), 1.0, 0.0).astype(BF)
    position = lax.broadcasted_iota(jnp.int32, (SEQ, GW), 0)
    inverse = 1.0 / jnp.minimum(position + 1, window).astype(F32)
    ps_all = ps_v[...].astype(F32)
    gw_all = gw_v[...]
    ps = jnp.zeros((1, GW), F32)
    gw = jnp.zeros((1, GW), F32)
    for g in range(NY):
        here = y == g
        ps = ps + jnp.where(here, ps_all[g : g + 1], 0.0)
        gw = gw + jnp.where(here, gw_all[g : g + 1], 0.0)

    def pool_body(i, carry):
        rows = pl.ds(pl.multiple_of(i * SEQ, SEQ), SEQ)
        p = pooled_v[rows, :]
        pf = p.astype(F32)
        sums = jnp.dot(band, p, preferred_element_type=F32)
        residual = (sums * inverse - pf).astype(BF)
        pool_v[rows, :] = jnp.dot(residual, wm_v[...], preferred_element_type=F32) * ps
        gate_v[rows, :] = 1.0 / (1.0 + jnp.exp(-(pf * gw)))
        return carry

    lax.fori_loop(0, ROWS // SEQ, pool_body, 0)

    for d in (0, 1):
        z_advance(d, 1, 1)

    ids_own.wait()
    for r in (1, 2, 3):
        remote(ids_h, idv.at[r], ids_ss.at[r], ids_rs.at[r], dev(dx=r)).wait_recv()
    ids_load = local(idv, ids_s, lsem.at[11])
    ids_load.wait()

    for d in (0, 1):
        q_copy(d, 1 - d, False).wait_recv()
    for d in (0, 1):
        z_advance(d, 0, 2)
    for d in (0, 1):
        z_advance(d, 1, 2)
    for d in (0, 1):
        q_copy(d, 2, False).wait_recv()
    for o in range(NZ):
        if o != 4:
            core_wait(0, o)
    z_advance(0, 0, 3)
    core_wait(0, 4)

    scale = hs_s[y] * (1.0 / math.sqrt(HD))
    eye = row_id == col_id

    def slot_of(r, b, j):
        p = ids_s[r, b, j]
        owner = lax.div(p, OWN)
        zo = lax.div(owner, NX * NC)
        xo = lax.rem(lax.div(owner, NC), NX)
        co = lax.rem(owner, NC)
        return (zo * NC + co) * OWN + lax.rem(p, OWN), xo == x

    def score_pair(r, pair):
        totals = []
        for u in (0, 1):
            b = pair * 2 + u
            q = qg_v[r, pl.ds(pl.multiple_of(b * BLOCK, BLOCK), BLOCK), :]
            found = [slot_of(r, b, j) for j in range(NPB)]
            kt = jnp.concatenate([kt_v[slot] for slot, _ in found], axis=1)
            sc = jnp.dot(q, kt, preferred_element_type=F32)
            e = jnp.exp(sc * scale)
            es = [
                jnp.where(found[j][1], e[:, j * PLEN : (j + 1) * PLEN], 0.0) for j in range(NPB)
            ]
            at = pl.multiple_of(b * BLOCK, BLOCK)
            for j in range(NPB):
                e_v[r, pl.ds(at, BLOCK), pl.ds(j * PLEN, PLEN)] = es[j].astype(BF)
            both = (es[0] + es[1]) + (es[2] + es[3])
            totals.append(jnp.sum(both, axis=1, keepdims=True))
        column = jnp.concatenate(totals, axis=0)
        row = jnp.sum(jnp.where(eye, column, 0.0), axis=0, keepdims=True)
        tot_v[r, pl.ds(pair, 1), :] = row

    for r in (2, 1, 3, 0):

        def score_body(i, carry, r=r):
            score_pair(r, i * 2)
            score_pair(r, i * 2 + 1)
            return carry

        lax.fori_loop(0, NBLK // 4, score_body, 0)
        if r:
            cp = remote(tot_v.at[r], totg_v.at[NX - r], ts.at[r], tr.at[NX - r], dev(dx=r))
            cp.start()
            sends.append(cp)

    for o in range(NZ):
        if o != 4:
            core_wait(1, o)
    z_advance(1, 1, 3)
    core_wait(1, 4)

    def value_quarter(r, quarter):
        def body(i, carry):
            for u in (0, 1):
                b = quarter * 4 + i * 2 + u
                at = pl.multiple_of(b * BLOCK, BLOCK)
                vv = jnp.concatenate([v_v[slot_of(r, b, j)[0]] for j in range(NPB)], axis=0)
                o = jnp.dot(e_v[r, pl.ds(at, BLOCK), :], vv, preferred_element_type=F32)
                part_v[r, pl.ds(at, BLOCK), :] = o.astype(BF)
            return carry

        lax.fori_loop(0, 2, body, 0)

    def rows_of(quarter):
        return pl.ds(quarter * QTR, QTR)

    def r_copy(d, m, src, dst):
        i = d * 6 + m
        return remote(src, dst, rs.at[i], rr.at[i], dev(dx=1 if d == 0 else -1))

    def r_send(d, m, src, dst):
        cp = r_copy(d, m, src, dst)
        cp.start()
        sends.append(cp)

    for step in (0, 1):
        for d in (0, 1):
            quarter = 2 * d + step
            value_quarter(2, quarter)
            r_send(
                d, step, part_v.at[2, rows_of(quarter)], rly_v.at[d, pl.ds(step * QTR, QTR)]
            )
    near = (1, 3)
    for step in (0, 1):
        for d in (0, 1):
            quarter = 2 * (1 - d) + step
            value_quarter(near[d], quarter)
            r_send(
                d, 2 + step, part_v.at[near[d], rows_of(quarter)], rrecv_v.at[d, rows_of(quarter)]
            )
    for step in (0, 1):
        for d in (0, 1):
            value_quarter(near[d], 2 * d + step)
    for step in (0, 1):
        for d in (0, 1):
            quarter = 2 * d + step
            here = pl.ds(step * QTR, QTR)
            r_copy(d, step, part_v.at[2, rows_of(quarter)], rly_v.at[d, here]).wait_recv()
            both = rly_v[d, here, :].astype(F32) + part_v[near[d], rows_of(quarter), :].astype(F32)
            sum_v[d, here, :] = both.astype(BF)
            r_send(d, 4 + step, sum_v.at[d, here], rrecv_v.at[d, rows_of(quarter)])
    for quarter in range(4):
        value_quarter(0, quarter)

    for r in (1, 2, 3):
        remote(tot_v.at[r], totg_v.at[r], ts.at[r], tr.at[r], dev(dx=r)).wait_recv()
    all_totals = tot_v[0] + totg_v[1] + totg_v[2] + totg_v[3]

    def y_copy(d, m, quarter, sending):
        sign = 1 if d == 0 else -1
        back = (0 if m < 4 else 1) + (0 if sending else 1)
        head = lax.rem(y - sign * back + NY, NY)
        block = att_v.at[head, rows_of(quarter)]
        i = d * 6 + m
        return remote(block, block, ys.at[i], yr.at[i], dev(dy=sign))

    order = (0, 2, 1, 3)
    for n, quarter in enumerate(order):
        step = quarter % 2
        for d in (0, 1):
            m = (4 + step) if d == quarter // 2 else (2 + step)
            r_copy(d, m, rrecv_v.at[d, rows_of(quarter)], rrecv_v.at[d, rows_of(quarter)]).wait_recv()
        columns = []
        for pair in range(2):
            row = all_totals[quarter * 2 + pair : quarter * 2 + pair + 1, :]
            columns.append(jnp.sum(jnp.where(eye, row, 0.0), axis=1, keepdims=True))
        total = jnp.concatenate(columns, axis=0)
        summed = (
            part_v[0, rows_of(quarter), :].astype(F32)
            + rrecv_v[0, rows_of(quarter), :].astype(F32)
            + rrecv_v[1, rows_of(quarter), :].astype(F32)
        )
        att_v[y, rows_of(quarter), :] = (summed * (1.0 / total)).astype(BF)
        for d in (0, 1):
            cp = y_copy(d, n, quarter, True)
            cp.start()
            sends.append(cp)

    for n, quarter in enumerate(order):
        d = quarter // 2
        y_copy(d, n, quarter, False).wait_recv()
        cp = y_copy(d, 4 + quarter % 2, quarter, True)
        cp.start()
        sends.append(cp)

    wc_own.wait()
    for r in (1, 2, 3):
        remote(
            wc_h.at[:, pl.ds(0, GW)], wc_v.at[lax.rem(y + r, NY)], wcs.at[r], wcr.at[r], dev(dy=r)
        ).wait_recv()
    wc = wc_v[...].reshape(NY * HD, GW)

    outs = []
    for n, quarter in enumerate(order):
        d = quarter // 2
        y_copy(1 - d, n, quarter, False).wait_recv()
        y_copy(d, 4 + quarter % 2, quarter, False).wait_recv()
        att = jnp.concatenate([att_v[h, rows_of(quarter), :] for h in range(NY)], axis=1)
        cross = jnp.dot(att, wc, preferred_element_type=F32)
        mixed = pool_v[rows_of(quarter), :] + gate_v[rows_of(quarter), :] * cross
        out_v[rows_of(quarter), :] = mixed.astype(BF)
        outs.append(local(out_v.at[rows_of(quarter)], out_h.at[rows_of(quarter)], osem.at[n]))

    for cp in sends:
        cp.wait_send()
    for cp in outs:
        cp.wait()


def per_device(
    tokens, passage_ids, store, mix_gain, w_query, w_key, w_value, w_cross_out,
    head_scale, w_pool_in, w_pool_mix, pool_scale, gate_weight,
):
    anywhere = pl.BlockSpec(memory_space=pl.ANY)
    dma = pltpu.SemaphoreType.DMA
    in_specs = [anywhere] * 13
    in_specs[8] = pl.BlockSpec(memory_space=pltpu.SMEM)
    v = pltpu.VMEM
    return pl.pallas_call(
        kernel,
        out_shape=jax.ShapeDtypeStruct((ROWS, GW), BF),
        in_specs=in_specs,
        out_specs=anywhere,
        scratch_shapes=[
            v((ROWS, D), BF),
            v((OWN, PLEN, D), BF),
            v((D, 2 * HD), BF),
            v((D, HD), BF),
            v((D, GW), BF),
            v((GW, GW), BF),
            v((1, D), BF),
            v((NY, GW), BF),
            v((NY, GW), F32),
            v((SLOTS, HD, PLEN), BF),
            v((SLOTS, PLEN, HD), BF),
            v((NX, ROWS, HD), BF),
            v((NX, NBLK, NPB), jnp.int32),
            pltpu.SMEM((NX, NBLK, NPB), jnp.int32),
            v((NY, HD, GW), BF),
            v((ROWS, GW), BF),
            v((ROWS, GW), F32),
            v((ROWS, GW), F32),
            v((NX, ROWS, NPB * PLEN), BF),
            v((NX, ROWS, HD), BF),
            v((2, ROWS // 2, HD), BF),
            v((2, ROWS // 2, HD), BF),
            v((2, ROWS, HD), BF),
            v((NX, 8, 128), F32),
            v((NX, 8, 128), F32),
            v((NY, ROWS, HD), BF),
            v((ROWS, GW), BF),
            dma((12,)),
            dma((ROWS // TCHUNK,)),
            dma((4,)),
            dma((16,)), dma((16,)),
            dma((16,)), dma((16,)),
            dma((6,)), dma((6,)),
            dma((4,)), dma((4,)),
            dma((4,)), dma((4,)),
            dma((4,)), dma((4,)),
            dma((12,)), dma((12,)),
            dma((12,)), dma((12,)),
        ],
        compiler_params=pltpu.CompilerParams(
            collective_id=0, has_side_effects=True, vmem_limit_bytes=60 * 1024 * 1024
        ),
        name="mixer",
    )(
        tokens, passage_ids, store, mix_gain.reshape(1, D), w_query, w_key, w_value, w_cross_out,
        head_scale, w_pool_in, w_pool_mix, pool_scale.reshape(NY, GW), gate_weight.reshape(NY, GW),
    )


def solution(mesh):
    return jax.shard_map(
        per_device,
        mesh=mesh,
        in_specs=(
            P("st", None),
            P("st", None),
            P("st", None, None),
            P(),
            P(None, "tp"),
            P(None, "tp"),
            P(None, "tp"),
            P("tp", None),
            P(),
            P(None, "tp"),
            P(),
            P(),
            P(),
        ),
        out_specs=P("st", "tp"),
        check_vma=False,
    )
```

```python
import functools
import math

import jax
import jax.numpy as jnp
from jax import lax
from jax.experimental import pallas as pl
from jax.experimental.pallas import tpu as pltpu
from jax.sharding import PartitionSpec as P

MESH = pl.DeviceIdType.MESH
BF = jnp.bfloat16
F32 = jnp.float32

EPSILON = 1e-06
NZ, NX, NC, NY = 8, 4, 2, 4
D = 4096
HD = 128
GW = 256
ROWS = 1024
BLOCK = 64
NPB = 4
NBLK = 16
PLEN = 128
OWN = 3
SEQ = 128
SLOTS = NZ * NC * OWN
TCHUNK = 256
STEP = 128

Z_ORDER = tuple(
    tuple((n // 100, n // 10 % 10, n % 10) for n in codes)
    for codes in (
        (1, 0, 101, 2, 100, 10, 11, 12, 102, 20, 21, 110, 22, 30, 31, 111, 112, 120, 121, 122, 130),
        (1, 0, 2, 102, 101, 10, 12, 11, 100, 111, 22, 21, 20, 112, 32, 121, 110, 122, 131, 120, 132),
    )
)


def kernel(
    tok_h, ids_h, store_h, gain_h, wq_h, wk_h, wv_h, wc_h, hs_s, wp_h, wm_h, ps_h, gw_h,
    out_h,
    tok_v, store_v, wkv_v, wqp_v, wm_v, gain_v, ps_v, gw_v,
    kt_v, v_v, qg_v, idv, tbl_v, tbl_s, wc_v,
    pooled_v, pool_v, gate_v, e_v, part_v, rly_v, sum_v, rrecv_v, tot_v, totg_v, att_v, out_v,
    lsem, tsem, osem,
    zs, zr, cs, cr, qs, qr, ids_ss, ids_rs, wcs, wcr, ts, tr, rs, rr, ys, yr,
):
    s = lax.axis_index("st")
    y = lax.axis_index("tp")
    c = lax.rem(s, NC)
    x = lax.rem(lax.div(s, NC), NX)
    z = lax.div(s, NC * NX)

    def dev(dz=0, dx=0, dy=0, other=False):
        cc = 1 - c if other else c
        zz = lax.rem(z + dz + NZ, NZ)
        xx = lax.rem(x + dx + NX, NX)
        yy = lax.rem(y + dy + NY, NY)
        return (zz * (NX * NC) + xx * NC + cc, yy)

    def remote(src, dst, ssem, rsem, to):
        return pltpu.make_async_remote_copy(
            src_ref=src, dst_ref=dst, send_sem=ssem, recv_sem=rsem,
            device_id=to, device_id_type=MESH,
        )

    barrier = pltpu.get_barrier_semaphore()
    partners = [
        dev(dz=1), dev(dz=-1), dev(dx=1), dev(dx=-1), dev(dx=2),
        dev(dy=1), dev(dy=-1), dev(dy=2), dev(other=True),
    ]
    for to in partners:
        pl.semaphore_signal(barrier, inc=1, device_id=to, device_id_type=MESH)

    def local(src, dst, sem):
        copy = pltpu.make_async_copy(src, dst, sem)
        copy.start()
        return copy

    kv_loads = []
    for h in (0, 1):
        part = pl.ds(h * (D // 2), D // 2)
        kv_loads.append([
            local(wk_h.at[part], wkv_v.at[part, pl.ds(0, HD)], lsem.at[3 * h]),
            local(wv_h.at[part], wkv_v.at[part, pl.ds(HD, HD)], lsem.at[3 * h + 1]),
            local(store_h.at[:, :, part], store_v.at[:, :, part], lsem.at[3 * h + 2]),
        ])

    def kv_half(h):
        half = slice(h * (D // 2), (h + 1) * (D // 2))
        return jnp.dot(
            store_v[:, :, half].reshape(OWN * PLEN, D // 2), wkv_v[half, :],
            preferred_element_type=F32,
        )

    for load in kv_loads[0]:
        load.wait()
    kv = kv_half(0)
    for load in kv_loads[1]:
        load.wait()
    gain_load = local(gain_h, gain_v, lsem.at[6])
    wq_load = local(wq_h, wqp_v.at[:, pl.ds(0, HD)], lsem.at[7])
    wp_load = local(wp_h, wqp_v.at[:, pl.ds(HD, GW)], lsem.at[8])
    tok_loads = []
    for i in range(ROWS // TCHUNK):
        chunk = pl.ds(i * TCHUNK, TCHUNK)
        tok_loads.append(local(tok_h.at[chunk], tok_v.at[chunk], tsem.at[i]))
    pool_loads = [
        local(wm_h.at[y], wm_v, lsem.at[9]),
        local(ps_h, ps_v, lsem.at[10]),
        local(gw_h, gw_v, lsem.at[11]),
    ]
    ids_own = local(ids_h, idv.at[0], lsem.at[12])
    wc_own = local(
        wc_h.at[:, pl.ds(pl.multiple_of(y * GW, GW), GW)], wc_v.at[y], lsem.at[13]
    )
    kv = kv + kv_half(1)
    keys = kv[:, :HD]
    keys = keys * lax.rsqrt(jnp.mean(keys * keys, axis=-1, keepdims=True) + EPSILON)
    own_slot = (z * NC + c) * OWN
    for i in range(OWN):
        rows = slice(i * PLEN, (i + 1) * PLEN)
        kt_v[own_slot + i] = jnp.transpose(keys[rows]).astype(BF)
        v_v[own_slot + i] = kv[rows, HD:].astype(BF)

    pl.semaphore_wait(barrier, len(partners))
    sends = []
    bufs = (kt_v, v_v)

    last = (((0, 0), (0, 1), (1, 0)), ((0, 2), (1, 1), (1, 2)))

    def z_copy(d, item, sending):
        kind, k, i = item
        sign = 1 if d == 0 else -1
        origin = lax.rem(z - sign * (k if sending else k + 1) + NZ, NZ)
        block = bufs[kind].at[(origin * NC + c) * OWN + i]
        n = ((d * 2 + kind) * 4 + k) * OWN + i
        return remote(block, block, zs.at[n], zr.at[n], dev(dz=sign))

    def core_copy(kind, o, core):
        block = bufs[kind].at[pl.ds((lax.rem(z + o, NZ) * NC + core) * OWN, OWN)]
        n = kind * NZ + o
        return remote(block, block, cs.at[n], cr.at[n], dev(other=True))

    def core_send(kind, o):
        cp = core_copy(kind, o, c)
        cp.start()
        sends.append(cp)

    arrived = set()

    def z_wait(d, item):
        if (d, item) in arrived:
            return
        arrived.add((d, item))
        z_copy(d, item, False).wait_recv()
        kind, k, _ = item
        if k < 3:
            if all((d, (kind, k, i)) in arrived for i in range(OWN)):
                core_send(kind, k + 1 if d == 1 else NZ - k - 1)
        elif all(
            (dd, (kind, 3, i)) in arrived for dd in (0, 1) for kk, i in last[dd] if kk == kind
        ):
            core_send(kind, 4)

    def z_step(n):
        for d in (0, 1):
            item = Z_ORDER[d][n]
            kind, k, i = item
            if k:
                z_wait(d, (kind, k - 1, i))
            cp = z_copy(d, item, True)
            cp.start()
            sends.append(cp)

    def z_finish(kind):
        for k in (2, 3):
            for d in (0, 1):
                for i in range(OWN):
                    if k == 2 or (kind, i) in last[d]:
                        z_wait(d, (kind, k, i))
        for o in range(NZ):
            core_copy(kind, o, 1 - c).wait_recv()

    for n in range(5):
        z_step(n)
    for kind in (0, 1):
        core_send(kind, 0)

    for r in (1, 2, 3):
        cp = remote(ids_h, idv.at[NX - r], ids_ss.at[r], ids_rs.at[NX - r], dev(dx=r))
        cp.start()
        sends.append(cp)
    for r in (1, 2, 3):
        column = pl.multiple_of(lax.rem(y + r, NY) * GW, GW)
        cp = remote(
            wc_h.at[:, pl.ds(column, GW)], wc_v.at[y], wcs.at[r], wcr.at[NY - r], dev(dy=r)
        )
        cp.start()
        sends.append(cp)

    gain_load.wait()
    wq_load.wait()
    wp_load.wait()
    gain = gain_v[...].reshape(1, D)

    def q_copy(d, m, sending):
        sign = 1 if d == 0 else -1
        if m < 2:
            half, back = m, 0
        else:
            half, back = d, 1
        origin = back if sending else back + 1
        row = (origin if d == 1 else NX - origin) % NX
        at = qg_v.at[row, pl.ds(half * (ROWS // 2), ROWS // 2)]
        back_there = back + 1
        row_there = (back_there if d == 1 else NX - back_there) % NX
        to = qg_v.at[row_there, pl.ds(half * (ROWS // 2), ROWS // 2)] if sending else at
        i = d * 3 + m
        return remote(at, to, qs.at[i], qr.at[i], dev(dx=sign))

    def q_send(d, m):
        cp = q_copy(d, m, True)
        cp.start()
        sends.append(cp)

    def token_chunk(i):
        tok_loads[i].wait()
        chunk = pl.ds(i * TCHUNK, TCHUNK)
        t = tok_v[chunk, :]
        tf = t.astype(F32)
        scale = lax.rsqrt(jnp.mean(tf * tf, axis=-1, keepdims=True) + EPSILON)
        both = jnp.dot(t * gain, wqp_v[...], preferred_element_type=F32) * scale
        q = both[:, :HD]
        q = q * lax.rsqrt(jnp.mean(q * q, axis=-1, keepdims=True) + EPSILON)
        qg_v[0, chunk, :] = q.astype(BF)
        pooled_v[chunk, :] = both[:, HD:].astype(BF)

    token_chunk(0)
    token_chunk(1)
    for d in (0, 1):
        q_send(d, 0)
    for n in (5, 6, 7, 8):
        z_step(n)
    token_chunk(2)
    for n in (9, 10):
        z_step(n)
    token_chunk(3)
    for d in (0, 1):
        q_send(d, 1)
    ids_own.wait()
    for r in (1, 2, 3):
        remote(ids_h, idv.at[r], ids_ss.at[r], ids_rs.at[r], dev(dx=r)).wait_recv()
    p = idv[...]
    owner = lax.shift_right_logical(p * 171, 9)
    place = lax.shift_right_logical(owner, 3) * NC + (owner & 1)
    tbl_v[0] = place * OWN + (p - owner * OWN)
    tbl_v[1] = jnp.where((lax.shift_right_logical(owner, 1) & 3) == x, 1, 0)
    tbl_load = local(tbl_v, tbl_s, lsem.at[14])
    for n in (11, 12, 13, 14):
        z_step(n)
    q_copy(0, 0, False).wait_recv()
    q_send(0, 2)
    tbl_load.wait()
    for n in (15, 16, 17):
        z_step(n)
    z_finish(0)
    q_copy(1, 1, False).wait_recv()
    q_send(1, 2)
    scale = hs_s[y] * (math.log2(math.e) / math.sqrt(HD))
    row_id = lax.broadcasted_iota(jnp.int32, (SEQ, SEQ), 0)
    col_id = lax.broadcasted_iota(jnp.int32, (SEQ, SEQ), 1)
    eye = row_id == col_id

    def slot_of(r, b, j):
        return tbl_s[0, r, j, b], tbl_s[1, r, j, b] == 1

    def score_pair(r, pair):
        totals = []
        for u in (0, 1):
            b = pair * 2 + u
            q = qg_v[r, pl.ds(pl.multiple_of(b * BLOCK, BLOCK), BLOCK), :]
            found = [slot_of(r, b, j) for j in range(NPB)]
            kt = jnp.concatenate([kt_v[slot] for slot, _ in found], axis=1)
            sc = jnp.dot(q, kt, preferred_element_type=F32)
            e = jnp.exp2(sc * scale)
            es = [
                jnp.where(found[j][1], e[:, j * PLEN : (j + 1) * PLEN], 0.0) for j in range(NPB)
            ]
            at = pl.multiple_of(b * BLOCK, BLOCK)
            for j in range(NPB):
                e_v[r, pl.ds(at, BLOCK), pl.ds(j * PLEN, PLEN)] = es[j].astype(BF)
            both = (es[0] + es[1]) + (es[2] + es[3])
            totals.append(jnp.sum(both, axis=1, keepdims=True))
        column = jnp.concatenate(totals, axis=0)
        row = jnp.sum(jnp.where(eye, column, 0.0), axis=0, keepdims=True)
        tot_v[r, pl.ds(pair, 1), :] = row

    def score_all(r):
        def score_body(i, carry):
            for u in range(4):
                score_pair(r, i * 4 + u)
            return carry

        lax.fori_loop(0, NBLK // 8, score_body, 0)
        if r:
            cp = remote(tot_v.at[r], totg_v.at[NX - r], ts.at[r], tr.at[NX - r], dev(dx=r))
            cp.start()
            sends.append(cp)

    score_all(0)
    z_step(18)
    q_copy(1, 0, False).wait_recv()
    score_all(1)
    z_step(19)
    q_copy(0, 1, False).wait_recv()
    score_all(3)
    z_step(20)
    for d in (0, 1):
        q_copy(d, 2, False).wait_recv()
    score_all(2)
    z_finish(1)

    def step_rows(d, i):
        return pl.ds(d * (ROWS // 2) + i * STEP, STEP)

    def values(pairs):
        for r, d, i in pairs:
            for u in range(STEP // BLOCK):
                b = d * (NBLK // 2) + i * (STEP // BLOCK) + u
                rows = pl.ds(b * BLOCK, BLOCK)
                vv = jnp.concatenate([v_v[slot_of(r, b, j)[0]] for j in range(NPB)], axis=0)
                o = jnp.dot(e_v[r, rows, :], vv, preferred_element_type=F32)
                part_v[r, rows, :] = o.astype(BF)

    def r_copy(d, m, i, src, dst):
        n = (d * 3 + m) * 4 + i
        return remote(src, dst, rs.at[n], rr.at[n], dev(dx=1 if d == 0 else -1))

    def r_send(d, m, i, src, dst):
        cp = r_copy(d, m, i, src, dst)
        cp.start()
        sends.append(cp)

    near = (1, 3)

    def far(i):
        values([(2, 0, i), (2, 1, i)])
        for d in (0, 1):
            here = pl.ds(i * STEP, STEP)
            r_send(d, 0, i, part_v.at[2, step_rows(d, i)], rly_v.at[d, here])

    def direct(i):
        values([(near[0], 1, i), (near[1], 0, i)])
        for d in (0, 1):
            rows = step_rows(1 - d, i)
            r_send(d, 1, i, part_v.at[near[d], rows], rrecv_v.at[d, rows])

    def relayed(i):
        values([(near[0], 0, i), (near[1], 1, i)])

    def own(i):
        values([(0, 0, i), (0, 1, i)])

    def relay(i):
        for d in (0, 1):
            rows = step_rows(d, i)
            here = pl.ds(i * STEP, STEP)
            r_copy(d, 0, i, part_v.at[2, rows], rly_v.at[d, here]).wait_recv()
            both = rly_v[d, here, :].astype(F32) + part_v[near[d], rows, :].astype(F32)
            sum_v[d, here, :] = both.astype(BF)
            r_send(d, 2, i, sum_v.at[d, here], rrecv_v.at[d, rows])

    def y_copy(d, m, half, i, sending):
        sign = 1 if d == 0 else -1
        back = (0 if m < 2 else 1) + (0 if sending else 1)
        head = lax.rem(y - sign * back + NY, NY)
        block = att_v.at[head, step_rows(half, i)]
        n = (d * 3 + m) * 4 + i
        return remote(block, block, ys.at[n], yr.at[n], dev(dy=sign))

    def y_send(d, m, half, i):
        cp = y_copy(d, m, half, i, True)
        cp.start()
        sends.append(cp)

    def attend(i):
        for half in (0, 1):
            rows = step_rows(half, i)
            for d in (0, 1):
                m = 2 if d == half else 1
                r_copy(d, m, i, rrecv_v.at[d, rows], rrecv_v.at[d, rows]).wait_recv()
            pair = half * 4 + i
            row = tot_v[0, pair : pair + 1, :]
            for r in (1, 2, 3):
                row = row + totg_v[r, pair : pair + 1, :]
            total = jnp.sum(jnp.where(eye, row, 0.0), axis=1, keepdims=True)
            summed = (
                part_v[0, rows, :].astype(F32)
                + rrecv_v[0, rows, :].astype(F32)
                + rrecv_v[1, rows, :].astype(F32)
            )
            att_v[y, rows, :] = (summed * (1.0 / total)).astype(BF)
            for d in (0, 1):
                y_send(d, half, half, i)

    def y_forward(i):
        for d in (0, 1):
            y_copy(d, d, d, i, False).wait_recv()
            y_send(d, 2, d, i)

    far(0)
    far(1)
    direct(0)
    relayed(0)
    far(2)
    relay(0)
    direct(1)
    relayed(1)
    far(3)
    relay(1)
    direct(2)
    relayed(2)
    own(0)
    relay(2)
    direct(3)
    relayed(3)
    own(1)
    for r in (1, 2, 3):
        remote(tot_v.at[r], totg_v.at[r], ts.at[r], tr.at[r], dev(dx=r)).wait_recv()
    attend(0)
    relay(3)
    own(2)
    own(3)
    for load in pool_loads:
        load.wait()
    window = lax.shift_left(jnp.int32(2), y.astype(jnp.int32))
    band = jnp.where((col_id <= row_id) & (col_id > row_id - window), 1.0, 0.0).astype(BF)
    position = lax.broadcasted_iota(jnp.int32, (SEQ, GW), 0)
    inverse = 1.0 / jnp.minimum(position + 1, window).astype(F32)
    ps_all = ps_v[...].astype(F32).reshape(1, NY * GW)
    gw_all = gw_v[...].reshape(1, NY * GW)
    ps = jnp.zeros((1, GW), F32)
    gw = jnp.zeros((1, GW), F32)
    for g in range(NY):
        here = y == g
        ps = ps + jnp.where(here, ps_all[:, g * GW : (g + 1) * GW], 0.0)
        gw = gw + jnp.where(here, gw_all[:, g * GW : (g + 1) * GW], 0.0)

    def pool_step(i):
        rows = pl.ds(i * SEQ, SEQ)
        p = pooled_v[rows, :]
        pf = p.astype(F32)
        sums = jnp.dot(band, p, preferred_element_type=F32)
        residual = (sums * inverse - pf).astype(BF)
        pool_v[rows, :] = jnp.dot(residual, wm_v[...], preferred_element_type=F32) * ps
        gate_v[rows, :] = 1.0 / (1.0 + jnp.exp(-(pf * gw)))

    pool_step(0)
    pool_step(4)
    attend(1)
    pool_step(1)
    pool_step(5)
    attend(2)
    y_forward(0)
    attend(3)
    y_forward(1)
    pool_step(2)
    pool_step(6)
    y_forward(2)
    pool_step(3)
    pool_step(7)
    wc_own.wait()
    for r in (1, 2, 3):
        remote(
            wc_h.at[:, pl.ds(0, GW)], wc_v.at[lax.rem(y + r, NY)], wcs.at[r], wcr.at[r], dev(dy=r)
        ).wait_recv()
    wc = wc_v[...].reshape(NY * HD, GW)

    outs = []

    def cross(i):
        for half in (0, 1):
            rows = step_rows(half, i)
            y_copy(1 - half, half, half, i, False).wait_recv()
            y_copy(half, 2, half, i, False).wait_recv()
            att = jnp.concatenate([att_v[h, rows, :] for h in range(NY)], axis=1)
            term = jnp.dot(att, wc, preferred_element_type=F32)
            mixed = pool_v[rows, :] + gate_v[rows, :] * term
            out_v[rows, :] = mixed.astype(BF)
            outs.append(local(out_v.at[rows], out_h.at[rows], osem.at[half * 4 + i]))

    cross(0)
    y_forward(3)
    cross(1)
    cross(2)
    cross(3)
    for cp in sends:
        cp.wait_send()
    for cp in outs:
        cp.wait()


def per_device(
    tokens, passage_ids, store, mix_gain, w_query, w_key, w_value, w_cross_out,
    head_scale, w_pool_in, w_pool_mix, pool_scale, gate_weight,
):
    anywhere = pl.BlockSpec(memory_space=pl.ANY)
    dma = pltpu.SemaphoreType.DMA
    in_specs = [anywhere] * 13
    in_specs[8] = pl.BlockSpec(memory_space=pltpu.SMEM)
    v = pltpu.VMEM
    return pl.pallas_call(
        kernel,
        out_shape=jax.ShapeDtypeStruct((ROWS, GW), BF),
        in_specs=in_specs,
        out_specs=anywhere,
        scratch_shapes=[
            v((ROWS, D), BF),
            v((OWN, PLEN, D), BF),
            v((D, 2 * HD), BF),
            v((D, HD + GW), BF),
            v((GW, GW), BF),
            v((D,), BF),
            v((NY * GW,), BF),
            v((NY * GW,), F32),
            v((SLOTS, HD, PLEN), BF),
            v((SLOTS, PLEN, HD), BF),
            v((NX, ROWS, HD), BF),
            v((NX, NPB, NBLK), jnp.int32),
            v((2, NX, NPB, NBLK), jnp.int32),
            pltpu.SMEM((2, NX, NPB, NBLK), jnp.int32),
            v((NY, HD, GW), BF),
            v((ROWS, GW), BF),
            v((ROWS, GW), F32),
            v((ROWS, GW), F32),
            v((NX, ROWS, NPB * PLEN), BF),
            v((NX, ROWS, HD), BF),
            v((2, ROWS // 2, HD), BF),
            v((2, ROWS // 2, HD), BF),
            v((2, ROWS, HD), BF),
            v((NX, 8, 128), F32),
            v((NX, 8, 128), F32),
            v((NY, ROWS, HD), BF),
            v((ROWS, GW), BF),
            dma((15,)),
            dma((ROWS // TCHUNK,)),
            dma((8,)),
            dma((48,)), dma((48,)),
            dma((16,)), dma((16,)),
            dma((6,)), dma((6,)),
            dma((4,)), dma((4,)),
            dma((4,)), dma((4,)),
            dma((4,)), dma((4,)),
            dma((24,)), dma((24,)),
            dma((24,)), dma((24,)),
        ],
        compiler_params=pltpu.CompilerParams(
            collective_id=0, has_side_effects=True, vmem_limit_bytes=60 * 1024 * 1024
        ),
        name="mixer",
    )(
        tokens, passage_ids.T, store, mix_gain, w_query, w_key, w_value, w_cross_out,
        head_scale, w_pool_in, w_pool_mix, pool_scale, gate_weight,
    )


def solution(mesh):
    return jax.shard_map(
        per_device,
        mesh=mesh,
        in_specs=(
            P("st", None),
            P("st", None),
            P("st", None, None),
            P(),
            P(None, "tp"),
            P(None, "tp"),
            P(None, "tp"),
            P("tp", None),
            P(),
            P(None, "tp"),
            P(),
            P(),
            P(),
        ),
        out_specs=P("st", "tp"),
        check_vma=False,
    )
```

```python
import functools
import math

import jax
import jax.numpy as jnp
from jax import lax
from jax.experimental import pallas as pl
from jax.experimental.pallas import tpu as pltpu
from jax.sharding import PartitionSpec as P

MESH = pl.DeviceIdType.MESH
BF = jnp.bfloat16
F32 = jnp.float32

EPSILON = 1e-06
NZ, NX, NC, NY = 8, 4, 2, 4
D = 4096
HD = 128
GW = 256
ROWS = 1024
BLOCK = 64
NPB = 4
NBLK = 16
PLEN = 128
OWN = 3
SEQ = 128
SLOTS = NZ * NC * OWN
TCHUNK = 256
PIECES = ROWS // TCHUNK * 2
KVP = 4
STEP = 128

SENT_ROWS = (
    42 * PLEN * HD + 16 * OWN * PLEN * HD + 6 * (ROWS // 2) * HD + 3 * HD * GW
    + 2 * 24 * STEP * HD
) // D

Z_ORDER = tuple(
    tuple((n // 100, n // 10 % 10, n % 10) for n in codes)
    for codes in (
        (1, 0, 101, 2, 100, 10, 11, 12, 102, 20, 21, 110, 22, 30, 31, 111, 112, 120, 121, 122, 130),
        (1, 0, 2, 102, 101, 10, 12, 11, 100, 111, 22, 21, 20, 112, 32, 121, 110, 122, 131, 120, 132),
    )
)


def kernel(
    tok_h, ids_h, store_h, gain_h, wq_h, wk_h, wv_h, wc_h, hs_s, wp_h, wm_h, ps_h, gw_h,
    out_h,
    tok_v, store_v, wkv_v, wqp_v, kv_v, acc_v, sq_v, wm_v, gain_v, ps_v, gw_v,
    kt_v, v_v, qg_v, idv, tbl_v, tbl_s, wc_v,
    pooled_v, pool_v, gate_v, e_v, part_v, rly_v, sum_v, rrecv_v, tot_v, totg_v, att_v, out_v,
    lsem, tsem, osem,
    ss, zr, cr, qr, ids_ss, ids_rs, wcr, ts, tr, rr, yr,
):
    s = lax.axis_index("st")
    y = lax.axis_index("tp")
    c = lax.rem(s, NC)
    x = lax.rem(lax.div(s, NC), NX)
    z = lax.div(s, NC * NX)

    def dev(dz=0, dx=0, dy=0, other=False):
        cc = 1 - c if other else c
        zz = lax.rem(z + dz + NZ, NZ)
        xx = lax.rem(x + dx + NX, NX)
        yy = lax.rem(y + dy + NY, NY)
        return (zz * (NX * NC) + xx * NC + cc, yy)

    def remote(src, dst, ssem, rsem, to):
        return pltpu.make_async_remote_copy(
            src_ref=src, dst_ref=dst, send_sem=ssem, recv_sem=rsem,
            device_id=to, device_id_type=MESH,
        )

    barrier = pltpu.get_barrier_semaphore()
    partners = [
        dev(dz=1, other=True), dev(dz=-1, other=True), dev(dx=1), dev(dx=-1), dev(dx=2),
        dev(dy=1), dev(dy=-1), dev(dy=2), dev(other=True),
    ]
    for to in partners:
        pl.semaphore_signal(barrier, inc=1, device_id=to, device_id_type=MESH)

    def local(src, dst, sem):
        copy = pltpu.make_async_copy(src, dst, sem)
        copy.start()
        return copy

    for h in range(KVP):
        part = pl.ds(h * (D // KVP), D // KVP)
        local(wk_h.at[part], wkv_v.at[part, pl.ds(0, HD)], lsem.at[2 * h])
        local(wv_h.at[part], wkv_v.at[part, pl.ds(HD, HD)], lsem.at[2 * h])
        local(store_h.at[:, :, part], store_v.at[:, :, part], lsem.at[2 * h + 1])

    def landed(ref, sem):
        pltpu.make_async_copy(ref, ref, sem).wait()

    def kv_part(h):
        part = pl.ds(h * (D // KVP), D // KVP)
        landed(wkv_v.at[part], lsem.at[2 * h])
        landed(store_v.at[:, :, part], lsem.at[2 * h + 1])
        term = jnp.dot(
            store_v[:, :, part].reshape(OWN * PLEN, D // KVP), wkv_v[part, :],
            preferred_element_type=F32,
        )
        kv_v[...] = term if h == 0 else kv_v[...] + term

    kv_part(0)
    kv_part(1)
    kv_part(2)
    kv_part(3)
    gain_load = local(gain_h, gain_v, lsem.at[8])
    local(wq_h, wqp_v.at[:, pl.ds(0, HD)], lsem.at[9])
    local(wp_h, wqp_v.at[:, pl.ds(HD, GW)], lsem.at[9])
    tok_loads = []
    for i in range(PIECES):
        part = (pl.ds(i // 2 * TCHUNK, TCHUNK), pl.ds(i % 2 * (D // 2), D // 2))
        tok_loads.append(local(tok_h.at[part], tok_v.at[part], tsem.at[i]))
    pool_loads = [
        local(wm_h.at[y], wm_v, lsem.at[10]),
        local(ps_h, ps_v, lsem.at[11]),
        local(gw_h, gw_v, lsem.at[12]),
    ]
    ids_own = local(ids_h, idv.at[0], lsem.at[13])
    wc_own = local(
        wc_h.at[:, pl.ds(pl.multiple_of(y * GW, GW), GW)], wc_v.at[y], lsem.at[14]
    )
    kv = kv_v[...]
    keys = kv[:, :HD]
    keys = keys * lax.rsqrt(jnp.mean(keys * keys, axis=-1, keepdims=True) + EPSILON)
    own_slot = (z * NC + c) * OWN
    for i in range(OWN):
        rows = slice(i * PLEN, (i + 1) * PLEN)
        kt_v[own_slot + i] = jnp.transpose(keys[rows]).astype(BF)
        v_v[own_slot + i] = kv[rows, HD:].astype(BF)

    pl.semaphore_wait(barrier, len(partners))
    bufs = (kt_v, v_v)

    last = (((0, 0), (0, 1), (1, 0)), ((0, 2), (1, 1), (1, 2)))

    def core_at(hops):
        return c if hops % 2 == 0 else 1 - c

    def z_copy(d, item, sending):
        kind, k, i = item
        sign = 1 if d == 0 else -1
        hops = k if sending else k + 1
        origin = lax.rem(z - sign * hops + NZ, NZ)
        block = bufs[kind].at[(origin * NC + core_at(hops)) * OWN + i]
        n = ((d * 2 + kind) * 4 + k) * OWN + i
        return remote(block, block, ss.at[0], zr.at[n], dev(dz=sign, other=True))

    def core_copy(kind, o):
        block = bufs[kind].at[pl.ds((lax.rem(z + o, NZ) * NC + core_at(o)) * OWN, OWN)]
        return remote(block, block, ss.at[0], cr.at[kind], dev(other=True))

    def core_send(kind, o):
        core_copy(kind, o).start()

    arrived = set()

    def z_wait(d, item):
        if (d, item) in arrived:
            return
        arrived.add((d, item))
        z_copy(d, item, False).wait_recv()
        kind, k, _ = item
        if k < 3:
            if all((d, (kind, k, i)) in arrived for i in range(OWN)):
                core_send(kind, k + 1 if d == 1 else NZ - k - 1)
        elif all(
            (dd, (kind, 3, i)) in arrived for dd in (0, 1) for kk, i in last[dd] if kk == kind
        ):
            core_send(kind, 4)

    def z_step(n):
        for d in (0, 1):
            item = Z_ORDER[d][n]
            kind, k, i = item
            if k:
                z_wait(d, (kind, k - 1, i))
            cp = z_copy(d, item, True)
            cp.start()

    def z_finish(kind):
        for k in (2, 3):
            for d in (0, 1):
                for i in range(OWN):
                    if k == 2 or (kind, i) in last[d]:
                        z_wait(d, (kind, k, i))

    def core_finish(kind):
        landed(bufs[kind].at[pl.ds(0, NZ * OWN)], cr.at[kind])

    for n in range(5):
        z_step(n)
    for kind in (0, 1):
        core_send(kind, 0)

    for r in (1, 2, 3):
        cp = remote(ids_h, idv.at[NX - r], ids_ss.at[0], ids_rs.at[0], dev(dx=r))
        cp.start()
    for r in (1, 2, 3):
        column = pl.multiple_of(lax.rem(y + r, NY) * GW, GW)
        cp = remote(
            wc_h.at[:, pl.ds(column, GW)], wc_v.at[y], ss.at[0], wcr.at[0], dev(dy=r)
        )
        cp.start()

    gain_load.wait()
    landed(wqp_v, lsem.at[9])
    gain = gain_v[...].reshape(1, D)

    def q_copy(d, m, sending):
        sign = 1 if d == 0 else -1
        if m < 2:
            half, back = m, 0
        else:
            half, back = d, 1
        origin = back if sending else back + 1
        row = (origin if d == 1 else NX - origin) % NX
        at = qg_v.at[row, pl.ds(half * (ROWS // 2), ROWS // 2)]
        back_there = back + 1
        row_there = (back_there if d == 1 else NX - back_there) % NX
        to = qg_v.at[row_there, pl.ds(half * (ROWS // 2), ROWS // 2)] if sending else at
        i = d * 3 + m
        return remote(at, to, ss.at[0], qr.at[i], dev(dx=sign))

    def q_send(d, m):
        cp = q_copy(d, m, True)
        cp.start()

    def token_piece(i):
        tok_loads[i].wait()
        rows = pl.ds(i // 2 * TCHUNK, TCHUNK)
        half = slice(i % 2 * (D // 2), (i % 2 + 1) * (D // 2))
        t = tok_v[rows, half]
        tf = t.astype(F32)
        squares = tf * tf
        folded = squares[:, :128]
        for n in range(1, D // 2 // 128):
            folded = folded + squares[:, n * 128 : (n + 1) * 128]
        term = jnp.dot(t * gain[:, half], wqp_v[half, :], preferred_element_type=F32)
        if i % 2 == 0:
            sq_v[...] = folded
            acc_v[...] = term
            return
        mean = jnp.sum(folded + sq_v[...], axis=-1, keepdims=True) * (1.0 / D)
        both = (term + acc_v[...]) * lax.rsqrt(mean + EPSILON)
        q = both[:, :HD]
        q = q * lax.rsqrt(jnp.mean(q * q, axis=-1, keepdims=True) + EPSILON)
        qg_v[0, rows, :] = q.astype(BF)
        pooled_v[rows, :] = both[:, HD:].astype(BF)

    for i in range(4):
        token_piece(i)
    for d in (0, 1):
        q_send(d, 0)
    z_step(5)
    z_step(6)
    token_piece(4)
    z_step(7)
    z_step(8)
    token_piece(5)
    z_step(9)
    token_piece(6)
    z_step(10)
    z_step(11)
    token_piece(7)
    for d in (0, 1):
        q_send(d, 1)
    z_step(12)
    ids_own.wait()
    landed(idv.at[pl.ds(0, NX - 1)], ids_rs.at[0])
    p = idv[...]
    owner = lax.shift_right_logical(p * 171, 9)
    place = lax.shift_right_logical(owner, 3) * NC + (owner & 1)
    tbl_v[0] = place * OWN + (p - owner * OWN)
    tbl_v[1] = jnp.where((lax.shift_right_logical(owner, 1) & 3) == x, 1, 0)
    tbl_load = local(tbl_v, tbl_s, lsem.at[15])
    for n in (13, 14):
        z_step(n)
    for n in (15, 16):
        z_step(n)
    tbl_load.wait()
    q_copy(0, 0, False).wait_recv()
    q_send(0, 2)
    z_step(17)
    z_finish(0)
    q_copy(1, 1, False).wait_recv()
    q_send(1, 2)
    core_finish(0)
    scale = hs_s[y] * (math.log2(math.e) / math.sqrt(HD))
    row_id = lax.broadcasted_iota(jnp.int32, (SEQ, SEQ), 0)
    col_id = lax.broadcasted_iota(jnp.int32, (SEQ, SEQ), 1)
    eye = row_id == col_id

    def slot_of(r, b, j):
        return tbl_s[0, r, j, b], tbl_s[1, r, j, b] == 1

    none = jnp.zeros((BLOCK, HD), BF)

    def score_pair(r, pair):
        b = (pair * 2, pair * 2 + 1)
        found = [[slot_of(r, n, j) for j in range(NPB)] for n in b]
        q = [qg_v[r, pl.ds(n * BLOCK, BLOCK), :] for n in b]
        left = jnp.concatenate(
            [jnp.concatenate([q[0], none], axis=1), jnp.concatenate([none, q[1]], axis=1)], axis=0
        )
        kt = jnp.concatenate(
            [jnp.concatenate([kt_v[slot] for slot, _ in f], axis=1) for f in found], axis=0
        )
        e = jnp.exp2(jnp.dot(left, kt, preferred_element_type=F32) * scale)
        totals = []
        for u in (0, 1):
            rows = slice(u * BLOCK, (u + 1) * BLOCK)
            es = [
                jnp.where(found[u][j][1], e[rows, j * PLEN : (j + 1) * PLEN], 0.0)
                for j in range(NPB)
            ]
            for j in range(NPB):
                e_v[r, pl.ds(b[u] * BLOCK, BLOCK), pl.ds(j * PLEN, PLEN)] = es[j].astype(BF)
            both = (es[0] + es[1]) + (es[2] + es[3])
            totals.append(jnp.sum(both, axis=1, keepdims=True))
        column = jnp.concatenate(totals, axis=0)
        row = jnp.sum(jnp.where(eye, column, 0.0), axis=0, keepdims=True)
        tot_v[r, pair : pair + 1, :] = row

    def score_group(r, half):
        for u in range(NBLK // 4):
            score_pair(r, half * (NBLK // 4) + u)
        if r and half:
            remote(tot_v.at[r], totg_v.at[NX - r], ts.at[0], tr.at[0], dev(dx=r)).start()

    score_group(0, 0)
    z_step(18)
    score_group(0, 1)
    z_step(19)
    q_copy(1, 0, False).wait_recv()
    score_group(1, 0)
    z_step(20)
    score_group(1, 1)
    q_copy(0, 1, False).wait_recv()
    score_group(3, 0)
    score_group(3, 1)
    for d in (0, 1):
        q_copy(d, 2, False).wait_recv()
    score_group(2, 0)
    z_finish(1)
    score_group(2, 1)
    core_finish(1)

    def step_rows(d, i):
        return pl.ds(d * (ROWS // 2) + i * STEP, STEP)

    def values(pairs):
        for r, d, i in pairs:
            b = d * (NBLK // 2) + i * (STEP // BLOCK)
            rows = pl.ds(b * BLOCK, STEP)
            vv = jnp.concatenate(
                [
                    jnp.concatenate([v_v[slot_of(r, b + u, j)[0]] for j in range(NPB)], axis=0)
                    for u in (0, 1)
                ],
                axis=1,
            )
            o = jnp.dot(e_v[r, rows, :], vv, preferred_element_type=F32)
            part_v[r, pl.ds(b * BLOCK, BLOCK), :] = o[:BLOCK, :HD].astype(BF)
            part_v[r, pl.ds((b + 1) * BLOCK, BLOCK), :] = o[BLOCK:, HD:].astype(BF)

    def r_copy(d, m, i, src, dst):
        n = i if m == 0 else 4 + i
        return remote(src, dst, ss.at[0], rr.at[n], dev(dx=1 if d == 0 else -1))

    def r_send(d, m, i, src, dst):
        cp = r_copy(d, m, i, src, dst)
        cp.start()

    near = (1, 3)

    def far(i):
        values([(2, 0, i), (2, 1, i)])
        for d in (0, 1):
            here = pl.ds(i * STEP, STEP)
            r_send(d, 0, i, part_v.at[2, step_rows(d, i)], rly_v.at[d, here])

    def direct(i):
        values([(near[0], 1, i), (near[1], 0, i)])
        for d in (0, 1):
            rows = step_rows(1 - d, i)
            r_send(d, 1, i, part_v.at[near[d], rows], rrecv_v.at[d, rows])

    def relayed(i):
        values([(near[0], 0, i), (near[1], 1, i)])

    def own(i):
        values([(0, 0, i), (0, 1, i)])

    def relay(i):
        landed(rly_v.at[:, pl.ds(0, STEP)], rr.at[i])
        for d in (0, 1):
            rows = step_rows(d, i)
            here = pl.ds(i * STEP, STEP)
            both = rly_v[d, here, :].astype(F32) + part_v[near[d], rows, :].astype(F32)
            sum_v[d, here, :] = both.astype(BF)
            r_send(d, 2, i, sum_v.at[d, here], rrecv_v.at[d, rows])

    def y_copy(d, m, half, i, sending):
        sign = 1 if d == 0 else -1
        back = (0 if m < 2 else 1) + (0 if sending else 1)
        head = lax.rem(y - sign * back + NY, NY)
        block = att_v.at[head, step_rows(half, i)]
        n = i if m == d else 4 + i
        return remote(block, block, ss.at[0], yr.at[n], dev(dy=sign))

    def y_send(d, m, half, i):
        cp = y_copy(d, m, half, i, True)
        cp.start()

    def attend(i):
        landed(rrecv_v.at[0, pl.ds(0, 4 * STEP)], rr.at[4 + i])
        for half in (0, 1):
            rows = step_rows(half, i)
            pair = half * 4 + i
            row = tot_v[0, pair : pair + 1, :]
            for r in (1, 2, 3):
                row = row + totg_v[r, pair : pair + 1, :]
            total = jnp.sum(jnp.where(eye, row, 0.0), axis=1, keepdims=True)
            summed = (
                part_v[0, rows, :].astype(F32)
                + rrecv_v[0, rows, :].astype(F32)
                + rrecv_v[1, rows, :].astype(F32)
            )
            att_v[y, rows, :] = (summed * (1.0 / total)).astype(BF)
            for d in (0, 1):
                y_send(d, half, half, i)

    def y_forward(i):
        landed(att_v.at[0, pl.ds(0, 2 * STEP)], yr.at[i])
        for d in (0, 1):
            y_send(d, 2, d, i)

    far(0)
    far(1)
    direct(0)
    relayed(0)
    far(2)
    relay(0)
    direct(1)
    relayed(1)
    far(3)
    relay(1)
    direct(2)
    relayed(2)
    own(0)
    relay(2)
    direct(3)
    relayed(3)
    own(1)
    landed(totg_v.at[pl.ds(1, NX - 1)], tr.at[0])
    attend(0)
    relay(3)
    own(2)
    own(3)
    for load in pool_loads:
        load.wait()
    window = lax.shift_left(jnp.int32(2), y.astype(jnp.int32))
    band = jnp.where((col_id <= row_id) & (col_id > row_id - window), 1.0, 0.0).astype(BF)
    position = lax.broadcasted_iota(jnp.int32, (SEQ, GW), 0)
    inverse = 1.0 / jnp.minimum(position + 1, window).astype(F32)
    ps_all = ps_v[...].astype(F32).reshape(1, NY * GW)
    gw_all = gw_v[...].reshape(1, NY * GW)
    ps = jnp.zeros((1, GW), F32)
    gw = jnp.zeros((1, GW), F32)
    for g in range(NY):
        here = y == g
        ps = ps + jnp.where(here, ps_all[:, g * GW : (g + 1) * GW], 0.0)
        gw = gw + jnp.where(here, gw_all[:, g * GW : (g + 1) * GW], 0.0)

    def pool_step(i):
        rows = pl.ds(i * SEQ, SEQ)
        p = pooled_v[rows, :]
        pf = p.astype(F32)
        sums = jnp.dot(band, p, preferred_element_type=F32)
        residual = (sums * inverse - pf).astype(BF)
        pool_v[rows, :] = jnp.dot(residual, wm_v[...], preferred_element_type=F32) * ps
        gate_v[rows, :] = 1.0 / (1.0 + jnp.exp(-(pf * gw)))

    pool_step(0)
    pool_step(4)
    attend(1)
    pool_step(1)
    pool_step(5)
    attend(2)
    y_forward(0)
    attend(3)
    y_forward(1)
    pool_step(2)
    pool_step(6)
    y_forward(2)
    pool_step(3)
    pool_step(7)
    wc_own.wait()
    landed(wc_v.at[pl.ds(0, NY - 1)], wcr.at[0])
    wc = wc_v[...].reshape(NY * HD, GW)

    def cross(i):
        landed(att_v.at[0, pl.ds(0, 4 * STEP)], yr.at[4 + i])
        for half in (0, 1):
            rows = step_rows(half, i)
            att = jnp.concatenate([att_v[h, rows, :] for h in range(NY)], axis=1)
            term = jnp.dot(att, wc, preferred_element_type=F32)
            mixed = pool_v[rows, :] + gate_v[rows, :] * term
            out_v[rows, :] = mixed.astype(BF)
            local(out_v.at[rows], out_h.at[rows], osem.at[0])

    cross(0)
    y_forward(3)
    cross(1)
    cross(2)
    cross(3)
    landed(idv.at[pl.ds(0, NX - 1)], ids_ss.at[0])
    landed(tot_v.at[pl.ds(0, NX - 1)], ts.at[0])
    landed(tok_v.at[pl.ds(0, SENT_ROWS)], ss.at[0])
    landed(out_v, osem.at[0])


def per_device(
    tokens, passage_ids, store, mix_gain, w_query, w_key, w_value, w_cross_out,
    head_scale, w_pool_in, w_pool_mix, pool_scale, gate_weight,
):
    anywhere = pl.BlockSpec(memory_space=pl.ANY)
    dma = pltpu.SemaphoreType.DMA
    in_specs = [anywhere] * 13
    in_specs[8] = pl.BlockSpec(memory_space=pltpu.SMEM)
    v = pltpu.VMEM
    return pl.pallas_call(
        kernel,
        out_shape=jax.ShapeDtypeStruct((ROWS, GW), BF),
        in_specs=in_specs,
        out_specs=anywhere,
        scratch_shapes=[
            v((ROWS, D), BF),
            v((OWN, PLEN, D), BF),
            v((D, 2 * HD), BF),
            v((D, HD + GW), BF),
            v((OWN * PLEN, 2 * HD), F32),
            v((TCHUNK, HD + GW), F32),
            v((TCHUNK, 128), F32),
            v((GW, GW), BF),
            v((D,), BF),
            v((NY * GW,), BF),
            v((NY * GW,), F32),
            v((SLOTS, HD, PLEN), BF),
            v((SLOTS, PLEN, HD), BF),
            v((NX, ROWS, HD), BF),
            v((NX, NPB, NBLK), jnp.int32),
            v((2, NX, NPB, NBLK), jnp.int32),
            pltpu.SMEM((2, NX, NPB, NBLK), jnp.int32),
            v((NY, HD, GW), BF),
            v((ROWS, GW), BF),
            v((ROWS, GW), F32),
            v((ROWS, GW), F32),
            v((NX, ROWS, NPB * PLEN), BF),
            v((NX, ROWS, HD), BF),
            v((2, ROWS // 2, HD), BF),
            v((2, ROWS // 2, HD), BF),
            v((2, ROWS, HD), BF),
            v((NX, 8, 128), F32),
            v((NX, 8, 128), F32),
            v((NY, ROWS, HD), BF),
            v((ROWS, GW), BF),
            dma((16,)),
            dma((PIECES,)),
            dma((1,)),
            dma((1,)),
            dma((48,)),
            dma((2,)),
            dma((6,)),
            dma((1,)), dma((1,)),
            dma((1,)),
            dma((1,)), dma((1,)),
            dma((8,)),
            dma((8,)),
        ],
        compiler_params=pltpu.CompilerParams(
            collective_id=0, has_side_effects=True, vmem_limit_bytes=60 * 1024 * 1024
        ),
        name="mixer",
    )(
        tokens, passage_ids.T, store, mix_gain, w_query, w_key, w_value, w_cross_out,
        head_scale, w_pool_in, w_pool_mix, pool_scale, gate_weight,
    )


def solution(mesh):
    return jax.shard_map(
        per_device,
        mesh=mesh,
        in_specs=(
            P("st", None),
            P("st", None),
            P("st", None, None),
            P(),
            P(None, "tp"),
            P(None, "tp"),
            P(None, "tp"),
            P("tp", None),
            P(),
            P(None, "tp"),
            P(),
            P(),
            P(),
        ),
        out_specs=P("st", "tp"),
        check_vma=False,
    )
```

```python
import functools
import math

import jax
import jax.numpy as jnp
from jax import lax
from jax.experimental import pallas as pl
from jax.experimental.pallas import tpu as pltpu
from jax.sharding import PartitionSpec as P

MESH = pl.DeviceIdType.MESH
BF = jnp.bfloat16
F32 = jnp.float32

EPSILON = 1e-06
NZ, NX, NC, NY = 8, 4, 2, 4
D = 4096
HD = 128
GW = 256
ROWS = 1024
BLOCK = 64
NPB = 4
NBLK = 16
PLEN = 128
OWN = 3
SEQ = 128
SLOTS = NZ * NC * OWN
TCHUNK = 256
PIECES = ROWS // TCHUNK * 2
KVP = 4
STEP = 128

SENT_ROWS = (
    42 * PLEN * HD + 16 * OWN * PLEN * HD + 6 * (ROWS // 2) * HD + 3 * HD * GW
    + 2 * 24 * STEP * HD
) // D

Z_ORDER = tuple(
    tuple((n // 100, n // 10 % 10, n % 10) for n in codes)
    for codes in (
        (1, 0, 101, 2, 100, 10, 11, 12, 102, 20, 21, 110, 22, 30, 31, 111, 112, 120, 121, 122, 130),
        (1, 0, 2, 102, 101, 10, 12, 11, 100, 111, 22, 21, 20, 112, 32, 121, 110, 122, 131, 120, 132),
    )
)


def kernel(
    tok_h, ids_h, store_h, gain_h, wq_h, wk_h, wv_h, wc_h, hs_s, wp_h, wm_h, ps_h, gw_h,
    out_v,
    tok_v, store_v, wkv_v, wqp_v, kv_v, acc_v, sq_v, wm_v, gain_v, ps_v, gw_v,
    kt_v, v_v, qg_v, idv, tbl_v, tbl_s, wc_v,
    pooled_v, pool_v, gate_v, e_v, part_v, rly_v, sum_v, rrecv_v, tot_v, totg_v, att_v,
    lsem, tsem,
    ss, zr, cr, qr, ids_ss, ids_rs, wcr, ts, tr, rr, yr,
):
    s = lax.axis_index("st")
    y = lax.axis_index("tp")
    c = lax.rem(s, NC)
    x = lax.rem(lax.div(s, NC), NX)
    z = lax.div(s, NC * NX)

    def dev(dz=0, dx=0, dy=0, other=False):
        cc = 1 - c if other else c
        zz = lax.rem(z + dz + NZ, NZ)
        xx = lax.rem(x + dx + NX, NX)
        yy = lax.rem(y + dy + NY, NY)
        return (zz * (NX * NC) + xx * NC + cc, yy)

    def remote(src, dst, ssem, rsem, to):
        return pltpu.make_async_remote_copy(
            src_ref=src, dst_ref=dst, send_sem=ssem, recv_sem=rsem,
            device_id=to, device_id_type=MESH,
        )

    barrier = pltpu.get_barrier_semaphore()
    partners = [
        dev(dz=1, other=True), dev(dz=-1, other=True), dev(dx=1), dev(dx=-1), dev(dx=2),
        dev(dy=1), dev(dy=-1), dev(dy=2), dev(other=True),
    ]
    for to in partners:
        pl.semaphore_signal(barrier, inc=1, device_id=to, device_id_type=MESH)

    def local(src, dst, sem):
        copy = pltpu.make_async_copy(src, dst, sem)
        copy.start()
        return copy

    for h in range(KVP):
        part = pl.ds(h * (D // KVP), D // KVP)
        local(wk_h.at[part], wkv_v.at[part, pl.ds(0, HD)], lsem.at[2 * h])
        local(wv_h.at[part], wkv_v.at[part, pl.ds(HD, HD)], lsem.at[2 * h])
        local(store_h.at[:, :, part], store_v.at[:, :, part], lsem.at[2 * h + 1])

    def landed(ref, sem):
        pltpu.make_async_copy(ref, ref, sem).wait()

    def kv_part(h):
        part = pl.ds(h * (D // KVP), D // KVP)
        landed(wkv_v.at[part], lsem.at[2 * h])
        landed(store_v.at[:, :, part], lsem.at[2 * h + 1])
        term = jnp.dot(
            store_v[:, :, part].reshape(OWN * PLEN, D // KVP), wkv_v[part, :],
            preferred_element_type=F32,
        )
        kv_v[...] = term if h == 0 else kv_v[...] + term

    kv_part(0)
    gain_load = local(gain_h, gain_v, lsem.at[8])
    local(wq_h, wqp_v.at[:, pl.ds(0, HD)], lsem.at[9])
    local(wp_h, wqp_v.at[:, pl.ds(HD, GW)], lsem.at[9])
    tok_loads = []

    def load_tokens(i):
        part = (pl.ds(i // 2 * TCHUNK, TCHUNK), pl.ds(i % 2 * (D // 2), D // 2))
        tok_loads.append(local(tok_h.at[part], tok_v.at[part], tsem.at[i]))

    for i in range(4):
        load_tokens(i)
    kv_part(1)
    kv_part(2)
    kv_part(3)
    for i in range(4, PIECES):
        load_tokens(i)
    pool_loads = [
        local(wm_h.at[y], wm_v, lsem.at[10]),
        local(ps_h, ps_v, lsem.at[11]),
        local(gw_h, gw_v, lsem.at[12]),
    ]
    ids_own = local(ids_h, idv.at[0], lsem.at[13])
    wc_own = local(
        wc_h.at[:, pl.ds(pl.multiple_of(y * GW, GW), GW)], wc_v.at[y], lsem.at[14]
    )
    kv = kv_v[...]
    keys = kv[:, :HD]
    keys = keys * lax.rsqrt(jnp.mean(keys * keys, axis=-1, keepdims=True) + EPSILON)
    own_slot = (z * NC + c) * OWN
    for i in range(OWN):
        rows = slice(i * PLEN, (i + 1) * PLEN)
        kt_v[own_slot + i] = jnp.transpose(keys[rows]).astype(BF)
        v_v[own_slot + i] = kv[rows, HD:].astype(BF)

    pl.semaphore_wait(barrier, len(partners))
    bufs = (kt_v, v_v)

    last = (((0, 0), (0, 1), (1, 0)), ((0, 2), (1, 1), (1, 2)))

    def core_at(hops):
        return c if hops % 2 == 0 else 1 - c

    def z_copy(d, item, sending):
        kind, k, i = item
        sign = 1 if d == 0 else -1
        hops = k if sending else k + 1
        origin = lax.rem(z - sign * hops + NZ, NZ)
        block = bufs[kind].at[(origin * NC + core_at(hops)) * OWN + i]
        n = ((d * 2 + kind) * 4 + k) * OWN + i
        return remote(block, block, ss.at[0], zr.at[n], dev(dz=sign, other=True))

    def core_copy(kind, o):
        block = bufs[kind].at[pl.ds((lax.rem(z + o, NZ) * NC + core_at(o)) * OWN, OWN)]
        return remote(block, block, ss.at[0], cr.at[kind], dev(other=True))

    def core_send(kind, o):
        core_copy(kind, o).start()

    arrived = set()

    def z_wait(d, item):
        if (d, item) in arrived:
            return
        arrived.add((d, item))
        z_copy(d, item, False).wait_recv()
        kind, k, _ = item
        if k < 3:
            if all((d, (kind, k, i)) in arrived for i in range(OWN)):
                core_send(kind, k + 1 if d == 1 else NZ - k - 1)
        elif all(
            (dd, (kind, 3, i)) in arrived for dd in (0, 1) for kk, i in last[dd] if kk == kind
        ):
            core_send(kind, 4)

    def z_step(n):
        for d in (0, 1):
            item = Z_ORDER[d][n]
            kind, k, i = item
            if k:
                z_wait(d, (kind, k - 1, i))
            cp = z_copy(d, item, True)
            cp.start()

    def z_finish(kind):
        for k in (2, 3):
            for d in (0, 1):
                for i in range(OWN):
                    if k == 2 or (kind, i) in last[d]:
                        z_wait(d, (kind, k, i))

    def core_finish(kind):
        landed(bufs[kind].at[pl.ds(0, NZ * OWN)], cr.at[kind])

    for n in range(5):
        z_step(n)
    for kind in (0, 1):
        core_send(kind, 0)

    for r in (1, 2, 3):
        cp = remote(ids_h, idv.at[NX - r], ids_ss.at[0], ids_rs.at[0], dev(dx=r))
        cp.start()
    for r in (1, 2, 3):
        column = pl.multiple_of(lax.rem(y + r, NY) * GW, GW)
        cp = remote(
            wc_h.at[:, pl.ds(column, GW)], wc_v.at[y], ss.at[0], wcr.at[0], dev(dy=r)
        )
        cp.start()

    gain_load.wait()
    landed(wqp_v, lsem.at[9])
    gain = gain_v[...].reshape(1, D)

    def q_copy(d, chunk, back):
        sign = 1 if d == 0 else -1
        rows = pl.ds(chunk * TCHUNK, TCHUNK)
        here = (-sign * back) % NX
        there = (-sign * (back + 1)) % NX
        if back:
            n = 3
        elif chunk % 2 == d:
            n = chunk // 2
        else:
            n = 2
        return remote(
            qg_v.at[here, rows], qg_v.at[there, rows], ss.at[0], qr.at[d * 4 + n], dev(dx=sign)
        )

    def q_send(chunk):
        for d in (0, 1):
            q_copy(d, chunk, 0).start()

    def q_forward(chunk):
        d = chunk % 2
        landed(qg_v.at[0, pl.ds(0, TCHUNK)], qr.at[d * 4 + chunk // 2])
        q_copy(d, chunk, 1).start()

    def q_pair(d, n):
        landed(qg_v.at[0, pl.ds(0, 2 * TCHUNK)], qr.at[d * 4 + n])

    def token_piece(i):
        tok_loads[i].wait()
        rows = pl.ds(i // 2 * TCHUNK, TCHUNK)
        half = slice(i % 2 * (D // 2), (i % 2 + 1) * (D // 2))
        t = tok_v[rows, half]
        tf = t.astype(F32)
        squares = tf * tf
        folded = squares[:, :128]
        for n in range(1, D // 2 // 128):
            folded = folded + squares[:, n * 128 : (n + 1) * 128]
        term = jnp.dot(t * gain[:, half], wqp_v[half, :], preferred_element_type=F32)
        if i % 2 == 0:
            sq_v[...] = folded
            acc_v[...] = term
            return
        mean = jnp.sum(folded + sq_v[...], axis=-1, keepdims=True) * (1.0 / D)
        both = (term + acc_v[...]) * lax.rsqrt(mean + EPSILON)
        q = both[:, :HD]
        q = q * lax.rsqrt(jnp.mean(q * q, axis=-1, keepdims=True) + EPSILON)
        qg_v[0, rows, :] = q.astype(BF)
        pooled_v[rows, :] = both[:, HD:].astype(BF)

    token_piece(0)
    token_piece(1)
    q_send(0)
    z_step(5)
    z_step(6)
    token_piece(2)
    z_step(7)
    z_step(8)
    token_piece(3)
    q_send(1)
    token_piece(4)
    z_step(9)
    z_step(10)
    token_piece(5)
    q_send(2)
    z_step(11)
    z_step(12)
    token_piece(6)
    token_piece(7)
    q_send(3)
    ids_own.wait()
    landed(idv.at[pl.ds(0, NX - 1)], ids_rs.at[0])
    p = idv[...]
    owner = lax.shift_right_logical(p * 171, 9)
    place = lax.shift_right_logical(owner, 3) * NC + (owner & 1)
    tbl_v[0] = place * OWN + (p - owner * OWN)
    tbl_v[1] = jnp.where((lax.shift_right_logical(owner, 1) & 3) == x, 1, 0)
    tbl_load = local(tbl_v, tbl_s, lsem.at[15])
    for n in (13, 14):
        z_step(n)
    for n in (15, 16):
        z_step(n)
    tbl_load.wait()
    q_forward(0)
    q_forward(1)
    z_step(17)
    q_forward(2)
    q_forward(3)
    z_finish(0)
    core_finish(0)
    scale = hs_s[y] * (math.log2(math.e) / math.sqrt(HD))
    row_id = lax.broadcasted_iota(jnp.int32, (SEQ, SEQ), 0)
    col_id = lax.broadcasted_iota(jnp.int32, (SEQ, SEQ), 1)
    eye = row_id == col_id

    def slot_of(r, b, j):
        return tbl_s[0, r, j, b], tbl_s[1, r, j, b] == 1

    none = jnp.zeros((BLOCK, HD), BF)

    def score_pair(r, pair):
        b = (pair * 2, pair * 2 + 1)
        found = [[slot_of(r, n, j) for j in range(NPB)] for n in b]
        q = [qg_v[r, pl.ds(n * BLOCK, BLOCK), :] for n in b]
        left = jnp.concatenate(
            [jnp.concatenate([q[0], none], axis=1), jnp.concatenate([none, q[1]], axis=1)], axis=0
        )
        kt = jnp.concatenate(
            [jnp.concatenate([kt_v[slot] for slot, _ in f], axis=1) for f in found], axis=0
        )
        e = jnp.exp2(jnp.dot(left, kt, preferred_element_type=F32) * scale)
        e = jnp.concatenate(
            [
                jnp.concatenate(
                    [
                        jnp.where(
                            found[u][j][1],
                            e[u * BLOCK : (u + 1) * BLOCK, j * PLEN : (j + 1) * PLEN], 0.0,
                        )
                        for j in range(NPB)
                    ],
                    axis=1,
                )
                for u in (0, 1)
            ],
            axis=0,
        )
        e_v[r, pl.ds(pair * 2 * BLOCK, 2 * BLOCK), :] = e.astype(BF)
        es = [e[:, j * PLEN : (j + 1) * PLEN] for j in range(NPB)]
        column = jnp.sum((es[0] + es[1]) + (es[2] + es[3]), axis=1, keepdims=True)
        row = jnp.sum(jnp.where(eye, column, 0.0), axis=0, keepdims=True)
        tot_v[r, pair : pair + 1, :] = row

    def score_group(r, half):
        for u in range(NBLK // 4):
            score_pair(r, half * (NBLK // 4) + u)
        if r and half:
            remote(tot_v.at[r], totg_v.at[NX - r], ts.at[0], tr.at[0], dev(dx=r)).start()

    score_group(0, 0)
    z_step(18)
    score_group(0, 1)
    z_step(19)
    q_pair(1, 2)
    score_group(1, 0)
    z_step(20)
    score_group(1, 1)
    q_pair(0, 2)
    score_group(3, 0)
    score_group(3, 1)
    for d in (0, 1):
        q_pair(d, 3)
    score_group(2, 0)
    z_finish(1)
    score_group(2, 1)
    core_finish(1)

    def step_rows(d, i):
        return pl.ds(d * (ROWS // 2) + i * STEP, STEP)

    def values(pairs):
        for r, d, i in pairs:
            b = d * (NBLK // 2) + i * (STEP // BLOCK)
            rows = pl.ds(b * BLOCK, STEP)
            vv = jnp.concatenate(
                [
                    jnp.concatenate([v_v[slot_of(r, b + u, j)[0]] for j in range(NPB)], axis=0)
                    for u in (0, 1)
                ],
                axis=1,
            )
            o = jnp.dot(e_v[r, rows, :], vv, preferred_element_type=F32)
            part_v[r, pl.ds(b * BLOCK, BLOCK), :] = o[:BLOCK, :HD].astype(BF)
            part_v[r, pl.ds((b + 1) * BLOCK, BLOCK), :] = o[BLOCK:, HD:].astype(BF)

    def r_copy(d, m, i, src, dst):
        n = i if m == 0 else 4 + i
        return remote(src, dst, ss.at[0], rr.at[n], dev(dx=1 if d == 0 else -1))

    def r_send(d, m, i, src, dst):
        cp = r_copy(d, m, i, src, dst)
        cp.start()

    near = (1, 3)

    def far(i):
        values([(2, 0, i), (2, 1, i)])
        for d in (0, 1):
            here = pl.ds(i * STEP, STEP)
            r_send(d, 0, i, part_v.at[2, step_rows(d, i)], rly_v.at[d, here])

    def direct(i):
        values([(near[0], 1, i), (near[1], 0, i)])
        for d in (0, 1):
            rows = step_rows(1 - d, i)
            r_send(d, 1, i, part_v.at[near[d], rows], rrecv_v.at[d, rows])

    def relayed(i):
        values([(near[0], 0, i), (near[1], 1, i)])

    def own(i):
        values([(0, 0, i), (0, 1, i)])

    def relay(i):
        landed(rly_v.at[:, pl.ds(0, STEP)], rr.at[i])
        for d in (0, 1):
            rows = step_rows(d, i)
            here = pl.ds(i * STEP, STEP)
            both = rly_v[d, here, :].astype(F32) + part_v[near[d], rows, :].astype(F32)
            sum_v[d, here, :] = both.astype(BF)
            r_send(d, 2, i, sum_v.at[d, here], rrecv_v.at[d, rows])

    def y_copy(d, m, half, i, sending):
        sign = 1 if d == 0 else -1
        back = (0 if m < 2 else 1) + (0 if sending else 1)
        head = lax.rem(y - sign * back + NY, NY)
        block = att_v.at[head, step_rows(half, i)]
        n = i if m == d else 4 + i
        return remote(block, block, ss.at[0], yr.at[n], dev(dy=sign))

    def y_send(d, m, half, i):
        cp = y_copy(d, m, half, i, True)
        cp.start()

    def attend(i):
        landed(rrecv_v.at[0, pl.ds(0, 4 * STEP)], rr.at[4 + i])
        for half in (0, 1):
            rows = step_rows(half, i)
            pair = half * 4 + i
            row = tot_v[0, pair : pair + 1, :]
            for r in (1, 2, 3):
                row = row + totg_v[r, pair : pair + 1, :]
            total = jnp.sum(jnp.where(eye, row, 0.0), axis=1, keepdims=True)
            summed = (
                part_v[0, rows, :].astype(F32)
                + rrecv_v[0, rows, :].astype(F32)
                + rrecv_v[1, rows, :].astype(F32)
            )
            att_v[y, rows, :] = (summed * (1.0 / total)).astype(BF)
            for d in (0, 1):
                y_send(d, half, half, i)

    def y_forward(i):
        landed(att_v.at[0, pl.ds(0, 2 * STEP)], yr.at[i])
        for d in (0, 1):
            y_send(d, 2, d, i)

    far(0)
    far(1)
    direct(0)
    relayed(0)
    far(2)
    relay(0)
    direct(1)
    relayed(1)
    far(3)
    relay(1)
    direct(2)
    relayed(2)
    own(0)
    relay(2)
    direct(3)
    relayed(3)
    own(1)
    landed(totg_v.at[pl.ds(1, NX - 1)], tr.at[0])
    attend(0)
    relay(3)
    own(2)
    own(3)
    for load in pool_loads:
        load.wait()
    window = lax.shift_left(jnp.int32(2), y.astype(jnp.int32))
    band = jnp.where((col_id <= row_id) & (col_id > row_id - window), 1.0, 0.0).astype(BF)
    position = lax.broadcasted_iota(jnp.int32, (SEQ, GW), 0)
    inverse = 1.0 / jnp.minimum(position + 1, window).astype(F32)
    ps_all = ps_v[...].astype(F32).reshape(1, NY * GW)
    gw_all = gw_v[...].reshape(1, NY * GW)
    ps = jnp.zeros((1, GW), F32)
    gw = jnp.zeros((1, GW), F32)
    for g in range(NY):
        here = y == g
        ps = ps + jnp.where(here, ps_all[:, g * GW : (g + 1) * GW], 0.0)
        gw = gw + jnp.where(here, gw_all[:, g * GW : (g + 1) * GW], 0.0)

    def pool_step(i):
        rows = pl.ds(i * SEQ, SEQ)
        p = pooled_v[rows, :]
        pf = p.astype(F32)
        sums = jnp.dot(band, p, preferred_element_type=F32)
        residual = (sums * inverse - pf).astype(BF)
        pool_v[rows, :] = jnp.dot(residual, wm_v[...], preferred_element_type=F32) * ps
        gate_v[rows, :] = 1.0 / (1.0 + jnp.exp(-(pf * gw)))

    pool_step(0)
    pool_step(4)
    attend(1)
    pool_step(1)
    pool_step(5)
    attend(2)
    y_forward(0)
    attend(3)
    y_forward(1)
    pool_step(2)
    pool_step(6)
    y_forward(2)
    pool_step(3)
    pool_step(7)
    wc_own.wait()
    landed(wc_v.at[pl.ds(0, NY - 1)], wcr.at[0])
    wc = wc_v[...].reshape(NY * HD, GW)

    def cross(i):
        landed(att_v.at[0, pl.ds(0, 4 * STEP)], yr.at[4 + i])
        for half in (0, 1):
            rows = step_rows(half, i)
            att = jnp.concatenate([att_v[h, rows, :] for h in range(NY)], axis=1)
            term = jnp.dot(att, wc, preferred_element_type=F32)
            mixed = pool_v[rows, :] + gate_v[rows, :] * term
            out_v[rows, :] = mixed.astype(BF)

    cross(0)
    y_forward(3)
    cross(1)
    cross(2)
    cross(3)
    landed(idv.at[pl.ds(0, NX - 1)], ids_ss.at[0])
    landed(tot_v.at[pl.ds(0, NX - 1)], ts.at[0])
    landed(tok_v.at[pl.ds(0, SENT_ROWS)], ss.at[0])


def per_device(
    tokens, passage_ids, store, mix_gain, w_query, w_key, w_value, w_cross_out,
    head_scale, w_pool_in, w_pool_mix, pool_scale, gate_weight,
):
    in_hbm = pl.BlockSpec(memory_space=pltpu.HBM)
    dma = pltpu.SemaphoreType.DMA
    in_specs = [in_hbm] * 13
    in_specs[8] = pl.BlockSpec(memory_space=pltpu.SMEM)
    v = pltpu.VMEM
    return pl.pallas_call(
        kernel,
        out_shape=jax.ShapeDtypeStruct((ROWS, GW), BF),
        in_specs=in_specs,
        out_specs=pl.BlockSpec(memory_space=pltpu.VMEM),
        scratch_shapes=[
            v((ROWS, D), BF),
            v((OWN, PLEN, D), BF),
            v((D, 2 * HD), BF),
            v((D, HD + GW), BF),
            v((OWN * PLEN, 2 * HD), F32),
            v((TCHUNK, HD + GW), F32),
            v((TCHUNK, 128), F32),
            v((GW, GW), BF),
            v((D,), BF),
            v((NY * GW,), BF),
            v((NY * GW,), F32),
            v((SLOTS, HD, PLEN), BF),
            v((SLOTS, PLEN, HD), BF),
            v((NX, ROWS, HD), BF),
            v((NX, NPB, NBLK), jnp.int32),
            v((2, NX, NPB, NBLK), jnp.int32),
            pltpu.SMEM((2, NX, NPB, NBLK), jnp.int32),
            v((NY, HD, GW), BF),
            v((ROWS, GW), BF),
            v((ROWS, GW), F32),
            v((ROWS, GW), F32),
            v((NX, ROWS, NPB * PLEN), BF),
            v((NX, ROWS, HD), BF),
            v((2, ROWS // 2, HD), BF),
            v((2, ROWS // 2, HD), BF),
            v((2, ROWS, HD), BF),
            v((NX, 8, 128), F32),
            v((NX, 8, 128), F32),
            v((NY, ROWS, HD), BF),
            dma((16,)),
            dma((PIECES,)),
            dma((1,)),
            dma((48,)),
            dma((2,)),
            dma((8,)),
            dma((1,)), dma((1,)),
            dma((1,)),
            dma((1,)), dma((1,)),
            dma((8,)),
            dma((8,)),
        ],
        compiler_params=pltpu.CompilerParams(
            collective_id=0, has_side_effects=True, vmem_limit_bytes=60 * 1024 * 1024
        ),
        name="mixer",
    )(
        tokens, passage_ids.T, store, mix_gain, w_query, w_key, w_value, w_cross_out,
        head_scale, w_pool_in, w_pool_mix, pool_scale, gate_weight,
    )


def solution(mesh):
    return jax.shard_map(
        per_device,
        mesh=mesh,
        in_specs=(
            P("st", None),
            P("st", None),
            P("st", None, None),
            P(),
            P(None, "tp"),
            P(None, "tp"),
            P(None, "tp"),
            P("tp", None),
            P(),
            P(None, "tp"),
            P(),
            P(),
            P(),
        ),
        out_specs=P("st", "tp"),
        check_vma=False,
    )
```

```python
import functools
import math

import jax
import jax.numpy as jnp
from jax import lax
from jax.experimental import pallas as pl
from jax.experimental.pallas import tpu as pltpu
from jax.sharding import PartitionSpec as P

MESH = pl.DeviceIdType.MESH
BF = jnp.bfloat16
F32 = jnp.float32

EPSILON = 1e-06
NZ, NX, NC, NY = 8, 4, 2, 4
D = 4096
HD = 128
GW = 256
ROWS = 1024
BLOCK = 64
NPB = 4
NBLK = 16
PLEN = 128
OWN = 3
SEQ = 128
SLOTS = NZ * NC * OWN
TCHUNK = 256
PIECES = ROWS // TCHUNK * 2
KVP = 4
STEP = 128

SENT_ROWS = (
    42 * PLEN * HD + 16 * OWN * PLEN * HD + 6 * (ROWS // 2) * HD + 3 * HD * GW
    + 2 * 24 * STEP * HD
) // D

Z_ORDER = tuple(
    tuple((n // 100, n // 10 % 10, n % 10) for n in codes)
    for codes in (
        (0, 1, 102, 2, 101, 100, 10, 11, 12, 111, 110, 20, 21, 112, 22, 120, 30, 31, 122, 121, 130),
        (2, 1, 100, 101, 0, 102, 12, 11, 111, 110, 112, 10, 22, 121, 21, 122, 20, 32, 120, 131, 132),
    )
)


def kernel(
    tok_h, ids_h, store_h, gain_h, wq_h, wk_h, wv_h, wc_h, hs_s, wp_h, wm_h, ps_h, gw_h,
    out_v,
    tok_v, store_v, wkv_v, wqp_v, kv_v, acc_v, sq_v, wm_v, gain_v, ps_v, gw_v,
    kt_v, v_v, qg_v, idv, tbl_v, tbl_s, wc_v,
    pooled_v, pool_v, gate_v, e_v, part_v, rly_v, sum_v, rrecv_v, tot_v, totg_v, att_v,
    lsem, tsem,
    ss, zr, cr, qr, ids_ss, ids_rs, wcr, ts, tr, rr, yr,
):
    s = lax.axis_index("st")
    y = lax.axis_index("tp")
    c = lax.rem(s, NC)
    x = lax.rem(lax.div(s, NC), NX)
    z = lax.div(s, NC * NX)

    def dev(dz=0, dx=0, dy=0, other=False):
        cc = 1 - c if other else c
        zz = lax.rem(z + dz + NZ, NZ)
        xx = lax.rem(x + dx + NX, NX)
        yy = lax.rem(y + dy + NY, NY)
        return (zz * (NX * NC) + xx * NC + cc, yy)

    def remote(src, dst, ssem, rsem, to):
        return pltpu.make_async_remote_copy(
            src_ref=src, dst_ref=dst, send_sem=ssem, recv_sem=rsem,
            device_id=to, device_id_type=MESH,
        )

    barrier = pltpu.get_barrier_semaphore()
    partners = [
        dev(dz=1, other=True), dev(dz=-1, other=True), dev(dx=1), dev(dx=-1), dev(dx=2),
        dev(dy=1), dev(dy=-1), dev(dy=2), dev(other=True),
    ]
    for to in partners:
        pl.semaphore_signal(barrier, inc=1, device_id=to, device_id_type=MESH)

    def local(src, dst, sem):
        copy = pltpu.make_async_copy(src, dst, sem)
        copy.start()
        return copy

    for h in range(KVP):
        part = pl.ds(h * (D // KVP), D // KVP)
        local(wk_h.at[part], wkv_v.at[part, pl.ds(0, HD)], lsem.at[2 * h])
        local(wv_h.at[part], wkv_v.at[part, pl.ds(HD, HD)], lsem.at[2 * h])
        local(store_h.at[:, :, part], store_v.at[:, :, part], lsem.at[2 * h + 1])

    def landed(ref, sem):
        pltpu.make_async_copy(ref, ref, sem).wait()

    def kv_part(h):
        part = pl.ds(h * (D // KVP), D // KVP)
        landed(wkv_v.at[part], lsem.at[2 * h])
        landed(store_v.at[:, :, part], lsem.at[2 * h + 1])
        term = jnp.dot(
            store_v[:, :, part].reshape(OWN * PLEN, D // KVP), wkv_v[part, :],
            preferred_element_type=F32,
        )
        kv_v[...] = term if h == 0 else kv_v[...] + term

    kv_part(0)
    gain_load = local(gain_h, gain_v, lsem.at[8])
    tok_loads = []

    def load_tokens(i):
        part = (pl.ds(i // 2 * TCHUNK, TCHUNK), pl.ds(i % 2 * (D // 2), D // 2))
        tok_loads.append(local(tok_h.at[part], tok_v.at[part], tsem.at[i]))

    for i in range(4):
        if i < 2:
            part = pl.ds(i * (D // 2), D // 2)
            local(wq_h.at[part], wqp_v.at[part, pl.ds(0, HD)], lsem.at[9 if i == 0 else 16])
            local(wp_h.at[part], wqp_v.at[part, pl.ds(HD, GW)], lsem.at[9 if i == 0 else 16])
        load_tokens(i)
    kv_part(1)
    kv_part(2)
    kv_part(3)
    for i in range(4, PIECES):
        load_tokens(i)
    pool_loads = [
        local(wm_h.at[y], wm_v, lsem.at[10]),
        local(ps_h, ps_v, lsem.at[11]),
        local(gw_h, gw_v, lsem.at[12]),
    ]
    ids_own = local(ids_h, idv.at[0], lsem.at[13])
    wc_own = local(
        wc_h.at[:, pl.ds(pl.multiple_of(y * GW, GW), GW)], wc_v.at[y], lsem.at[14]
    )
    kv = kv_v[...]
    keys = kv[:, :HD]
    keys = keys * lax.rsqrt(jnp.mean(keys * keys, axis=-1, keepdims=True) + EPSILON)
    own_slot = (z * NC + c) * OWN
    for i in range(OWN):
        rows = slice(i * PLEN, (i + 1) * PLEN)
        kt_v[own_slot + i] = jnp.transpose(keys[rows]).astype(BF)
        v_v[own_slot + i] = kv[rows, HD:].astype(BF)

    pl.semaphore_wait(barrier, len(partners))
    bufs = (kt_v, v_v)

    last = (((0, 0), (0, 1), (1, 0)), ((0, 2), (1, 1), (1, 2)))

    def core_at(hops):
        return c if hops % 2 == 0 else 1 - c

    def z_copy(d, item, sending):
        kind, k, i = item
        sign = 1 if d == 0 else -1
        hops = k if sending else k + 1
        origin = lax.rem(z - sign * hops + NZ, NZ)
        block = bufs[kind].at[(origin * NC + core_at(hops)) * OWN + i]
        n = ((d * 2 + kind) * 4 + k) * OWN + i
        return remote(block, block, ss.at[0], zr.at[n], dev(dz=sign, other=True))

    def core_copy(kind, o):
        block = bufs[kind].at[pl.ds((lax.rem(z + o, NZ) * NC + core_at(o)) * OWN, OWN)]
        return remote(block, block, ss.at[0], cr.at[kind], dev(other=True))

    def core_send(kind, o):
        core_copy(kind, o).start()

    arrived = set()

    def z_wait(d, item):
        if (d, item) in arrived:
            return
        arrived.add((d, item))
        z_copy(d, item, False).wait_recv()
        kind, k, _ = item
        if k < 3:
            if all((d, (kind, k, i)) in arrived for i in range(OWN)):
                core_send(kind, k + 1 if d == 1 else NZ - k - 1)
        elif all(
            (dd, (kind, 3, i)) in arrived for dd in (0, 1) for kk, i in last[dd] if kk == kind
        ):
            core_send(kind, 4)

    def z_step(n):
        for d in (0, 1):
            item = Z_ORDER[d][n]
            kind, k, i = item
            if k:
                z_wait(d, (kind, k - 1, i))
            cp = z_copy(d, item, True)
            cp.start()

    def z_finish(kind):
        for k in (2, 3):
            for d in (0, 1):
                for i in range(OWN):
                    if k == 2 or (kind, i) in last[d]:
                        z_wait(d, (kind, k, i))

    def core_finish(kind):
        landed(bufs[kind].at[pl.ds(0, NZ * OWN)], cr.at[kind])

    for n in range(6):
        z_step(n)
    for kind in (0, 1):
        core_send(kind, 0)

    for r in (1, 2, 3):
        cp = remote(ids_h, idv.at[NX - r], ids_ss.at[0], ids_rs.at[0], dev(dx=r))
        cp.start()
    for r in (1, 2, 3):
        column = pl.multiple_of(lax.rem(y + r, NY) * GW, GW)
        cp = remote(
            wc_h.at[:, pl.ds(column, GW)], wc_v.at[y], ss.at[0], wcr.at[0], dev(dy=r)
        )
        cp.start()

    gain_load.wait()
    gain = gain_v[...].reshape(1, D)

    def q_copy(d, chunk, back):
        sign = 1 if d == 0 else -1
        rows = pl.ds(chunk * TCHUNK, TCHUNK)
        here = (-sign * back) % NX
        there = (-sign * (back + 1)) % NX
        if back:
            n = 3
        elif chunk % 2 == d:
            n = chunk // 2
        else:
            n = 2
        return remote(
            qg_v.at[here, rows], qg_v.at[there, rows], ss.at[0], qr.at[d * 4 + n], dev(dx=sign)
        )

    def q_send(chunk):
        for d in (0, 1):
            q_copy(d, chunk, 0).start()

    def q_forward(chunk):
        d = chunk % 2
        landed(qg_v.at[0, pl.ds(0, TCHUNK)], qr.at[d * 4 + chunk // 2])
        q_copy(d, chunk, 1).start()

    def q_pair(d, n):
        landed(qg_v.at[0, pl.ds(0, 2 * TCHUNK)], qr.at[d * 4 + n])

    def token_piece(i):
        if i < 2:
            landed(wqp_v.at[pl.ds(i * (D // 2), D // 2)], lsem.at[9 if i == 0 else 16])
        tok_loads[i].wait()
        rows = pl.ds(i // 2 * TCHUNK, TCHUNK)
        half = slice(i % 2 * (D // 2), (i % 2 + 1) * (D // 2))
        t = tok_v[rows, half]
        tf = t.astype(F32)
        squares = tf * tf
        folded = squares[:, :128]
        for n in range(1, D // 2 // 128):
            folded = folded + squares[:, n * 128 : (n + 1) * 128]
        term = jnp.dot(t * gain[:, half], wqp_v[half, :], preferred_element_type=F32)
        if i % 2 == 0:
            sq_v[...] = folded
            acc_v[...] = term
            return
        mean = jnp.sum(folded + sq_v[...], axis=-1, keepdims=True) * (1.0 / D)
        both = (term + acc_v[...]) * lax.rsqrt(mean + EPSILON)
        q = both[:, :HD]
        q = q * lax.rsqrt(jnp.mean(q * q, axis=-1, keepdims=True) + EPSILON)
        qg_v[0, rows, :] = q.astype(BF)
        pooled_v[rows, :] = both[:, HD:].astype(BF)

    token_piece(0)
    token_piece(1)
    q_send(0)
    z_step(6)
    z_step(7)
    token_piece(2)
    token_piece(3)
    q_send(1)
    z_step(8)
    token_piece(4)
    z_step(9)
    token_piece(5)
    q_send(2)
    z_step(10)
    z_step(11)
    token_piece(6)
    z_step(12)
    token_piece(7)
    q_send(3)
    z_step(13)
    z_step(14)
    q_forward(0)
    ids_own.wait()
    landed(idv.at[pl.ds(0, NX - 1)], ids_rs.at[0])
    p = idv[...]
    owner = lax.shift_right_logical(p * 171, 9)
    place = lax.shift_right_logical(owner, 3) * NC + (owner & 1)
    tbl_v[0] = place * OWN + (p - owner * OWN)
    tbl_v[1] = jnp.where((lax.shift_right_logical(owner, 1) & 3) == x, 1, 0)
    tbl_load = local(tbl_v, tbl_s, lsem.at[15])
    z_step(15)
    q_forward(1)
    z_step(16)
    q_forward(2)
    z_step(17)
    tbl_load.wait()
    z_step(18)
    z_step(19)
    q_forward(3)
    z_step(20)
    z_finish(0)
    q_pair(1, 2)
    q_pair(0, 2)
    core_finish(0)
    scale = hs_s[y] * (math.log2(math.e) / math.sqrt(HD))
    row_id = lax.broadcasted_iota(jnp.int32, (SEQ, SEQ), 0)
    col_id = lax.broadcasted_iota(jnp.int32, (SEQ, SEQ), 1)
    eye = row_id == col_id

    def slot_of(r, b, j):
        return tbl_s[0, r, j, b], tbl_s[1, r, j, b] == 1

    none = jnp.zeros((BLOCK, HD), BF)

    def score_pair(r, pair):
        b = (pair * 2, pair * 2 + 1)
        found = [[slot_of(r, n, j) for j in range(NPB)] for n in b]
        q = [qg_v[r, pl.ds(n * BLOCK, BLOCK), :] for n in b]
        left = jnp.concatenate(
            [jnp.concatenate([q[0], none], axis=1), jnp.concatenate([none, q[1]], axis=1)], axis=0
        )
        kt = jnp.concatenate(
            [jnp.concatenate([kt_v[slot] for slot, _ in f], axis=1) for f in found], axis=0
        )
        e = jnp.exp2(jnp.dot(left, kt, preferred_element_type=F32) * scale)
        e = jnp.concatenate(
            [
                jnp.concatenate(
                    [
                        jnp.where(
                            found[u][j][1],
                            e[u * BLOCK : (u + 1) * BLOCK, j * PLEN : (j + 1) * PLEN], 0.0,
                        )
                        for j in range(NPB)
                    ],
                    axis=1,
                )
                for u in (0, 1)
            ],
            axis=0,
        )
        e_v[r, pl.ds(pair * 2 * BLOCK, 2 * BLOCK), :] = e.astype(BF)
        es = [e[:, j * PLEN : (j + 1) * PLEN] for j in range(NPB)]
        column = jnp.sum((es[0] + es[1]) + (es[2] + es[3]), axis=1, keepdims=True)
        row = jnp.sum(jnp.where(eye, column, 0.0), axis=0, keepdims=True)
        tot_v[r, pair : pair + 1, :] = row

    def score_group(r, half):
        for u in range(NBLK // 4):
            score_pair(r, half * (NBLK // 4) + u)
        if r and half:
            remote(tot_v.at[r], totg_v.at[NX - r], ts.at[0], tr.at[0], dev(dx=r)).start()

    score_group(0, 0)
    score_group(0, 1)
    score_group(1, 0)
    score_group(1, 1)
    z_finish(1)
    for d in (0, 1):
        q_pair(d, 3)
    score_group(3, 0)
    score_group(3, 1)
    score_group(2, 0)
    score_group(2, 1)
    core_finish(1)

    def step_rows(d, i):
        return pl.ds(d * (ROWS // 2) + i * STEP, STEP)

    def values(pairs):
        for r, d, i in pairs:
            b = d * (NBLK // 2) + i * (STEP // BLOCK)
            rows = pl.ds(b * BLOCK, STEP)
            vv = jnp.concatenate(
                [
                    jnp.concatenate([v_v[slot_of(r, b + u, j)[0]] for j in range(NPB)], axis=0)
                    for u in (0, 1)
                ],
                axis=1,
            )
            o = jnp.dot(e_v[r, rows, :], vv, preferred_element_type=F32)
            part_v[r, pl.ds(b * BLOCK, BLOCK), :] = o[:BLOCK, :HD].astype(BF)
            part_v[r, pl.ds((b + 1) * BLOCK, BLOCK), :] = o[BLOCK:, HD:].astype(BF)

    def r_copy(d, m, i, src, dst):
        n = i if m == 0 else 4 + i
        return remote(src, dst, ss.at[0], rr.at[n], dev(dx=1 if d == 0 else -1))

    def r_send(d, m, i, src, dst):
        cp = r_copy(d, m, i, src, dst)
        cp.start()

    near = (1, 3)

    def far(i):
        values([(2, 0, i), (2, 1, i)])
        for d in (0, 1):
            here = pl.ds(i * STEP, STEP)
            r_send(d, 0, i, part_v.at[2, step_rows(d, i)], rly_v.at[d, here])

    def direct(i):
        values([(near[0], 1, i), (near[1], 0, i)])
        for d in (0, 1):
            rows = step_rows(1 - d, i)
            r_send(d, 1, i, part_v.at[near[d], rows], rrecv_v.at[d, rows])

    def relayed(i):
        values([(near[0], 0, i), (near[1], 1, i)])

    def own(i):
        values([(0, 0, i), (0, 1, i)])

    def relay(i):
        landed(rly_v.at[:, pl.ds(0, STEP)], rr.at[i])
        for d in (0, 1):
            rows = step_rows(d, i)
            here = pl.ds(i * STEP, STEP)
            both = rly_v[d, here, :].astype(F32) + part_v[near[d], rows, :].astype(F32)
            sum_v[d, here, :] = both.astype(BF)
            r_send(d, 2, i, sum_v.at[d, here], rrecv_v.at[d, rows])

    def y_copy(d, m, half, i, sending):
        sign = 1 if d == 0 else -1
        back = (0 if m < 2 else 1) + (0 if sending else 1)
        head = lax.rem(y - sign * back + NY, NY)
        block = att_v.at[head, step_rows(half, i)]
        n = i if m == d else 4 + i
        return remote(block, block, ss.at[0], yr.at[n], dev(dy=sign))

    def y_send(d, m, half, i):
        cp = y_copy(d, m, half, i, True)
        cp.start()

    def attend(i):
        landed(rrecv_v.at[0, pl.ds(0, 4 * STEP)], rr.at[4 + i])
        for half in (0, 1):
            rows = step_rows(half, i)
            pair = half * 4 + i
            row = tot_v[0, pair : pair + 1, :]
            for r in (1, 2, 3):
                row = row + totg_v[r, pair : pair + 1, :]
            total = jnp.sum(jnp.where(eye, row, 0.0), axis=1, keepdims=True)
            summed = (
                part_v[0, rows, :].astype(F32)
                + rrecv_v[0, rows, :].astype(F32)
                + rrecv_v[1, rows, :].astype(F32)
            )
            att_v[y, rows, :] = (summed * (1.0 / total)).astype(BF)
            for d in (0, 1):
                y_send(d, half, half, i)

    def y_forward(i):
        landed(att_v.at[0, pl.ds(0, 2 * STEP)], yr.at[i])
        for d in (0, 1):
            y_send(d, 2, d, i)

    far(0)
    far(1)
    direct(0)
    relayed(0)
    far(2)
    relay(0)
    direct(1)
    relayed(1)
    far(3)
    relay(1)
    direct(2)
    relayed(2)
    own(0)
    relay(2)
    direct(3)
    relayed(3)
    own(1)
    landed(totg_v.at[pl.ds(1, NX - 1)], tr.at[0])
    attend(0)
    relay(3)
    own(2)
    own(3)
    for load in pool_loads:
        load.wait()
    window = lax.shift_left(jnp.int32(2), y.astype(jnp.int32))
    band = jnp.where((col_id <= row_id) & (col_id > row_id - window), 1.0, 0.0).astype(BF)
    position = lax.broadcasted_iota(jnp.int32, (SEQ, GW), 0)
    inverse = 1.0 / jnp.minimum(position + 1, window).astype(F32)
    ps_all = ps_v[...].astype(F32).reshape(1, NY * GW)
    gw_all = gw_v[...].reshape(1, NY * GW)
    ps = jnp.zeros((1, GW), F32)
    gw = jnp.zeros((1, GW), F32)
    for g in range(NY):
        here = y == g
        ps = ps + jnp.where(here, ps_all[:, g * GW : (g + 1) * GW], 0.0)
        gw = gw + jnp.where(here, gw_all[:, g * GW : (g + 1) * GW], 0.0)

    def pool_step(i):
        rows = pl.ds(i * SEQ, SEQ)
        p = pooled_v[rows, :]
        pf = p.astype(F32)
        sums = jnp.dot(band, p, preferred_element_type=F32)
        residual = (sums * inverse - pf).astype(BF)
        pool_v[rows, :] = jnp.dot(residual, wm_v[...], preferred_element_type=F32) * ps
        gate_v[rows, :] = 1.0 / (1.0 + jnp.exp(-(pf * gw)))

    pool_step(0)
    pool_step(4)
    attend(1)
    pool_step(1)
    pool_step(5)
    attend(2)
    y_forward(0)
    attend(3)
    y_forward(1)
    pool_step(2)
    pool_step(6)
    y_forward(2)
    pool_step(3)
    pool_step(7)
    wc_own.wait()
    landed(wc_v.at[pl.ds(0, NY - 1)], wcr.at[0])
    wc = wc_v[...].reshape(NY * HD, GW)

    def cross(i):
        landed(att_v.at[0, pl.ds(0, 4 * STEP)], yr.at[4 + i])
        for half in (0, 1):
            rows = step_rows(half, i)
            att = jnp.concatenate([att_v[h, rows, :] for h in range(NY)], axis=1)
            term = jnp.dot(att, wc, preferred_element_type=F32)
            mixed = pool_v[rows, :] + gate_v[rows, :] * term
            out_v[rows, :] = mixed.astype(BF)

    cross(0)
    y_forward(3)
    cross(1)
    cross(2)
    cross(3)
    landed(idv.at[pl.ds(0, NX - 1)], ids_ss.at[0])
    landed(tot_v.at[pl.ds(0, NX - 1)], ts.at[0])
    landed(tok_v.at[pl.ds(0, SENT_ROWS)], ss.at[0])


def per_device(
    tokens, passage_ids, store, mix_gain, w_query, w_key, w_value, w_cross_out,
    head_scale, w_pool_in, w_pool_mix, pool_scale, gate_weight,
):
    in_hbm = pl.BlockSpec(memory_space=pltpu.HBM)
    dma = pltpu.SemaphoreType.DMA
    in_specs = [in_hbm] * 13
    in_specs[8] = pl.BlockSpec(memory_space=pltpu.SMEM)
    v = pltpu.VMEM
    return pl.pallas_call(
        kernel,
        out_shape=jax.ShapeDtypeStruct((ROWS, GW), BF),
        in_specs=in_specs,
        out_specs=pl.BlockSpec(memory_space=pltpu.VMEM),
        scratch_shapes=[
            v((ROWS, D), BF),
            v((OWN, PLEN, D), BF),
            v((D, 2 * HD), BF),
            v((D, HD + GW), BF),
            v((OWN * PLEN, 2 * HD), F32),
            v((TCHUNK, HD + GW), F32),
            v((TCHUNK, 128), F32),
            v((GW, GW), BF),
            v((D,), BF),
            v((NY * GW,), BF),
            v((NY * GW,), F32),
            v((SLOTS, HD, PLEN), BF),
            v((SLOTS, PLEN, HD), BF),
            v((NX, ROWS, HD), BF),
            v((NX, NPB, NBLK), jnp.int32),
            v((2, NX, NPB, NBLK), jnp.int32),
            pltpu.SMEM((2, NX, NPB, NBLK), jnp.int32),
            v((NY, HD, GW), BF),
            v((ROWS, GW), BF),
            v((ROWS, GW), F32),
            v((ROWS, GW), F32),
            v((NX, ROWS, NPB * PLEN), BF),
            v((NX, ROWS, HD), BF),
            v((2, ROWS // 2, HD), BF),
            v((2, ROWS // 2, HD), BF),
            v((2, ROWS, HD), BF),
            v((NX, 8, 128), F32),
            v((NX, 8, 128), F32),
            v((NY, ROWS, HD), BF),
            dma((17,)),
            dma((PIECES,)),
            dma((1,)),
            dma((48,)),
            dma((2,)),
            dma((8,)),
            dma((1,)), dma((1,)),
            dma((1,)),
            dma((1,)), dma((1,)),
            dma((8,)),
            dma((8,)),
        ],
        compiler_params=pltpu.CompilerParams(
            collective_id=0, has_side_effects=True, vmem_limit_bytes=60 * 1024 * 1024
        ),
        name="mixer",
    )(
        tokens, passage_ids.T, store, mix_gain, w_query, w_key, w_value, w_cross_out,
        head_scale, w_pool_in, w_pool_mix, pool_scale, gate_weight,
    )


def solution(mesh):
    return jax.shard_map(
        per_device,
        mesh=mesh,
        in_specs=(
            P("st", None),
            P("st", None),
            P("st", None, None),
            P(),
            P(None, "tp"),
            P(None, "tp"),
            P(None, "tp"),
            P("tp", None),
            P(),
            P(None, "tp"),
            P(),
            P(),
            P(),
        ),
        out_specs=P("st", "tp"),
        check_vma=False,
    )
```

```python
import functools
import math

import jax
import jax.numpy as jnp
from jax import lax
from jax.experimental import pallas as pl
from jax.experimental.pallas import tpu as pltpu
from jax.sharding import PartitionSpec as P

MESH = pl.DeviceIdType.MESH
BF = jnp.bfloat16
F32 = jnp.float32

EPSILON = 1e-06
NZ, NX, NC, NY = 8, 4, 2, 4
D = 4096
HD = 128
GW = 256
ROWS = 1024
BLOCK = 64
NPB = 4
NBLK = 16
PLEN = 128
OWN = 3
SEQ = 128
SLOTS = NZ * NC * OWN
TCHUNK = 256
PIECES = ROWS // TCHUNK * 2
KVP = 4
STEP = 128

SENT_ROWS = (
    42 * PLEN * HD + 16 * OWN * PLEN * HD + 6 * (ROWS // 2) * HD + 3 * HD * GW
    + 2 * 24 * STEP * HD
) // D

Z_ORDER = tuple(
    tuple((n // 100, n // 10 % 10, n % 10) for n in codes)
    for codes in (
        (0, 1, 102, 2, 101, 100, 10, 11, 12, 111, 110, 20, 21, 112, 22, 120, 30, 31, 122, 121, 130),
        (2, 1, 100, 101, 0, 102, 12, 11, 111, 110, 112, 10, 22, 121, 21, 122, 20, 32, 120, 131, 132),
    )
)


def kernel(
    tok_h, ids_h, store_h, gain_h, wq_h, wk_h, wv_h, wc_h, hs_s, wp_h, wm_h, ps_h, gw_h,
    out_v,
    tok_v, store_v, wkv_v, wqp_v, kv_v, acc_v, sq_v, wm_v, gain_v, ps_v, gw_v,
    kt_v, v_v, qg_v, idv, tbl_v, tbl_s, wc_v,
    pooled_v, pool_v, gate_v, e_v, part_v, rly_v, sum_v, rrecv_v, tot_v, totg_v, att_v,
    lsem, tsem,
    ss, zr, cr, qr, ids_ss, ids_rs, wcr, ts, tr, rr, yr,
):
    s = lax.axis_index("st")
    y = lax.axis_index("tp")
    c = lax.rem(s, NC)
    x = lax.rem(lax.div(s, NC), NX)
    z = lax.div(s, NC * NX)

    def dev(dz=0, dx=0, dy=0, other=False):
        cc = 1 - c if other else c
        zz = lax.rem(z + dz + NZ, NZ)
        xx = lax.rem(x + dx + NX, NX)
        yy = lax.rem(y + dy + NY, NY)
        return (zz * (NX * NC) + xx * NC + cc, yy)

    def remote(src, dst, ssem, rsem, to):
        return pltpu.make_async_remote_copy(
            src_ref=src, dst_ref=dst, send_sem=ssem, recv_sem=rsem,
            device_id=to, device_id_type=MESH,
        )

    barrier = pltpu.get_barrier_semaphore()
    partners = [
        dev(dz=1, other=True), dev(dz=-1, other=True), dev(dx=1), dev(dx=-1), dev(dx=2),
        dev(dy=1), dev(dy=-1), dev(dy=2), dev(other=True),
    ]
    for to in partners:
        pl.semaphore_signal(barrier, inc=1, device_id=to, device_id_type=MESH)

    def local(src, dst, sem):
        copy = pltpu.make_async_copy(src, dst, sem)
        copy.start()
        return copy

    for h in range(KVP):
        part = pl.ds(h * (D // KVP), D // KVP)
        local(wk_h.at[part], wkv_v.at[part, pl.ds(0, HD)], lsem.at[2 * h])
        local(wv_h.at[part], wkv_v.at[part, pl.ds(HD, HD)], lsem.at[2 * h])
        local(store_h.at[:, :, part], store_v.at[:, :, part], lsem.at[2 * h + 1])

    def landed(ref, sem):
        pltpu.make_async_copy(ref, ref, sem).wait()

    def kv_part(h):
        part = pl.ds(h * (D // KVP), D // KVP)
        landed(wkv_v.at[part], lsem.at[2 * h])
        landed(store_v.at[:, :, part], lsem.at[2 * h + 1])
        term = jnp.dot(
            store_v[:, :, part].reshape(OWN * PLEN, D // KVP), wkv_v[part, :],
            preferred_element_type=F32,
        )
        kv_v[...] = term if h == 0 else kv_v[...] + term

    kv_part(0)
    gain_load = local(gain_h, gain_v, lsem.at[8])
    tok_loads = []

    def load_tokens(i):
        part = (pl.ds(i // 2 * TCHUNK, TCHUNK), pl.ds(i % 2 * (D // 2), D // 2))
        tok_loads.append(local(tok_h.at[part], tok_v.at[part], tsem.at[i]))

    for i in range(4):
        if i < 2:
            part = pl.ds(i * (D // 2), D // 2)
            local(wq_h.at[part], wqp_v.at[part, pl.ds(0, HD)], lsem.at[9 if i == 0 else 16])
            local(wp_h.at[part], wqp_v.at[part, pl.ds(HD, GW)], lsem.at[9 if i == 0 else 16])
        load_tokens(i)
    kv_part(1)
    kv_part(2)
    kv_part(3)
    for i in range(4, PIECES):
        load_tokens(i)
    pool_loads = [
        local(wm_h.at[y], wm_v, lsem.at[10]),
        local(ps_h, ps_v, lsem.at[11]),
        local(gw_h, gw_v, lsem.at[12]),
    ]
    ids_own = local(ids_h, idv.at[0], lsem.at[13])
    wc_own = local(
        wc_h.at[:, pl.ds(pl.multiple_of(y * GW, GW), GW)], wc_v.at[y], lsem.at[14]
    )
    kv = kv_v[...]
    keys = kv[:, :HD]
    keys = keys * lax.rsqrt(jnp.mean(keys * keys, axis=-1, keepdims=True) + EPSILON)
    own_slot = (z * NC + c) * OWN
    for i in range(OWN):
        rows = slice(i * PLEN, (i + 1) * PLEN)
        kt_v[own_slot + i] = jnp.transpose(keys[rows]).astype(BF)
        v_v[own_slot + i] = kv[rows, HD:].astype(BF)

    pl.semaphore_wait(barrier, len(partners))
    bufs = (kt_v, v_v)

    last = (((0, 0), (0, 1), (1, 0)), ((0, 2), (1, 1), (1, 2)))

    def core_at(hops):
        return c if hops % 2 == 0 else 1 - c

    def z_copy(d, item, sending):
        kind, k, i = item
        sign = 1 if d == 0 else -1
        hops = k if sending else k + 1
        origin = lax.rem(z - sign * hops + NZ, NZ)
        block = bufs[kind].at[(origin * NC + core_at(hops)) * OWN + i]
        onward = (kind, k + 1, i)
        n = Z_ORDER[d].index(onward) if onward in Z_ORDER[d] else len(Z_ORDER[d]) + kind
        return remote(block, block, ss.at[0], zr.at[n], dev(dz=sign, other=True))

    def core_copy(kind, o):
        block = bufs[kind].at[pl.ds((lax.rem(z + o, NZ) * NC + core_at(o)) * OWN, OWN)]
        return remote(block, block, ss.at[0], cr.at[kind], dev(other=True))

    def core_send(kind, o):
        core_copy(kind, o).start()

    arrived = set()

    def z_arrived(d, item):
        arrived.add((d, item))
        kind, k, _ = item
        if k < 3:
            if all((d, (kind, k, i)) in arrived for i in range(OWN)):
                core_send(kind, k + 1 if d == 1 else NZ - k - 1)
        elif all(
            (dd, (kind, 3, i)) in arrived for dd in (0, 1) for kk, i in last[dd] if kk == kind
        ):
            core_send(kind, 4)

    def z_step(n):
        if n >= 6:
            landed(kt_v.at[pl.ds(0, 2)], zr.at[n])
        for d in (0, 1):
            z_copy(d, Z_ORDER[d][n], True).start()
        for d in (0, 1):
            kind, k, i = Z_ORDER[d][n]
            if k:
                z_arrived(d, (kind, k - 1, i))

    def z_finish(kind):
        landed(kt_v.at[pl.ds(0, 6)], zr.at[len(Z_ORDER[0]) + kind])
        for k in (2, 3):
            for d in (0, 1):
                for i in range(OWN):
                    stays = (kind, i) in last[d] if k == 3 else (kind, i) not in last[d]
                    if stays:
                        z_arrived(d, (kind, k, i))

    def core_finish(kind):
        landed(bufs[kind].at[pl.ds(0, NZ * OWN)], cr.at[kind])

    for n in range(6):
        z_step(n)
    for kind in (0, 1):
        core_send(kind, 0)

    for r in (1, 2, 3):
        cp = remote(ids_h, idv.at[NX - r], ids_ss.at[0], ids_rs.at[0], dev(dx=r))
        cp.start()
    for r in (1, 2, 3):
        column = pl.multiple_of(lax.rem(y + r, NY) * GW, GW)
        cp = remote(
            wc_h.at[:, pl.ds(column, GW)], wc_v.at[y], ss.at[0], wcr.at[0], dev(dy=r)
        )
        cp.start()

    gain_load.wait()
    gain = gain_v[...].reshape(1, D)

    def q_copy(d, chunk, back):
        sign = 1 if d == 0 else -1
        rows = pl.ds(chunk * TCHUNK, TCHUNK)
        here = (-sign * back) % NX
        there = (-sign * (back + 1)) % NX
        if back:
            n = 3
        elif chunk % 2 == d:
            n = chunk // 2
        else:
            n = 2
        return remote(
            qg_v.at[here, rows], qg_v.at[there, rows], ss.at[0], qr.at[d * 4 + n], dev(dx=sign)
        )

    def q_send(chunk):
        for d in (0, 1):
            q_copy(d, chunk, 0).start()

    def q_forward(chunk):
        d = chunk % 2
        landed(qg_v.at[0, pl.ds(0, TCHUNK)], qr.at[d * 4 + chunk // 2])
        q_copy(d, chunk, 1).start()

    def q_pair(d, n):
        landed(qg_v.at[0, pl.ds(0, 2 * TCHUNK)], qr.at[d * 4 + n])

    def token_piece(i):
        if i < 2:
            landed(wqp_v.at[pl.ds(i * (D // 2), D // 2)], lsem.at[9 if i == 0 else 16])
        tok_loads[i].wait()
        rows = pl.ds(i // 2 * TCHUNK, TCHUNK)
        half = slice(i % 2 * (D // 2), (i % 2 + 1) * (D // 2))
        t = tok_v[rows, half]
        tf = t.astype(F32)
        squares = tf * tf
        folded = squares[:, :128]
        for n in range(1, D // 2 // 128):
            folded = folded + squares[:, n * 128 : (n + 1) * 128]
        term = jnp.dot(t * gain[:, half], wqp_v[half, :], preferred_element_type=F32)
        if i % 2 == 0:
            sq_v[...] = folded
            acc_v[...] = term
            return
        mean = jnp.sum(folded + sq_v[...], axis=-1, keepdims=True) * (1.0 / D)
        both = (term + acc_v[...]) * lax.rsqrt(mean + EPSILON)
        q = both[:, :HD]
        q = q * lax.rsqrt(jnp.mean(q * q, axis=-1, keepdims=True) + EPSILON)
        qg_v[0, rows, :] = q.astype(BF)
        pooled_v[rows, :] = both[:, HD:].astype(BF)

    token_piece(0)
    token_piece(1)
    q_send(0)
    z_step(6)
    z_step(7)
    token_piece(2)
    token_piece(3)
    q_send(1)
    z_step(8)
    token_piece(4)
    z_step(9)
    token_piece(5)
    q_send(2)
    z_step(10)
    z_step(11)
    token_piece(6)
    z_step(12)
    token_piece(7)
    q_send(3)
    z_step(13)
    z_step(14)
    q_forward(0)
    ids_own.wait()
    landed(idv.at[pl.ds(0, NX - 1)], ids_rs.at[0])
    p = idv[...]
    owner = lax.shift_right_logical(p * 171, 9)
    place = lax.shift_right_logical(owner, 3) * NC + (owner & 1)
    tbl_v[0] = place * OWN + (p - owner * OWN)
    tbl_v[1] = jnp.where((lax.shift_right_logical(owner, 1) & 3) == x, 1, 0)
    tbl_load = local(tbl_v, tbl_s, lsem.at[15])
    z_step(15)
    q_forward(1)
    z_step(16)
    q_forward(2)
    z_step(17)
    tbl_load.wait()
    z_step(18)
    z_step(19)
    q_forward(3)
    z_step(20)
    z_finish(0)
    q_pair(1, 2)
    q_pair(0, 2)
    core_finish(0)
    scale = hs_s[y] * (math.log2(math.e) / math.sqrt(HD))
    row_id = lax.broadcasted_iota(jnp.int32, (SEQ, SEQ), 0)
    col_id = lax.broadcasted_iota(jnp.int32, (SEQ, SEQ), 1)
    eye = row_id == col_id

    def slot_of(r, b, j):
        return tbl_s[0, r, j, b], tbl_s[1, r, j, b] == 1

    none = jnp.zeros((BLOCK, HD), BF)

    def score_pair(r, pair):
        b = (pair * 2, pair * 2 + 1)
        found = [[slot_of(r, n, j) for j in range(NPB)] for n in b]
        q = [qg_v[r, pl.ds(n * BLOCK, BLOCK), :] for n in b]
        left = jnp.concatenate(
            [jnp.concatenate([q[0], none], axis=1), jnp.concatenate([none, q[1]], axis=1)], axis=0
        )
        kt = jnp.concatenate(
            [jnp.concatenate([kt_v[slot] for slot, _ in f], axis=1) for f in found], axis=0
        )
        e = jnp.exp2(jnp.dot(left, kt, preferred_element_type=F32) * scale)
        e = jnp.concatenate(
            [
                jnp.concatenate(
                    [
                        jnp.where(
                            found[u][j][1],
                            e[u * BLOCK : (u + 1) * BLOCK, j * PLEN : (j + 1) * PLEN], 0.0,
                        )
                        for j in range(NPB)
                    ],
                    axis=1,
                )
                for u in (0, 1)
            ],
            axis=0,
        )
        e_v[r, pl.ds(pair * 2 * BLOCK, 2 * BLOCK), :] = e.astype(BF)
        es = [e[:, j * PLEN : (j + 1) * PLEN] for j in range(NPB)]
        column = jnp.sum((es[0] + es[1]) + (es[2] + es[3]), axis=1, keepdims=True)
        row = jnp.sum(jnp.where(eye, column, 0.0), axis=0, keepdims=True)
        tot_v[r, pair : pair + 1, :] = row

    def score_group(r, half):
        for u in range(NBLK // 4):
            score_pair(r, half * (NBLK // 4) + u)
        if r and half:
            remote(tot_v.at[r], totg_v.at[NX - r], ts.at[0], tr.at[0], dev(dx=r)).start()

    score_group(0, 0)
    score_group(0, 1)
    score_group(1, 0)
    score_group(1, 1)
    z_finish(1)
    for d in (0, 1):
        q_pair(d, 3)
    score_group(3, 0)
    score_group(3, 1)
    score_group(2, 0)
    score_group(2, 1)
    core_finish(1)

    def step_rows(d, i):
        return pl.ds(d * (ROWS // 2) + i * STEP, STEP)

    def values(pairs):
        for r, d, i in pairs:
            b = d * (NBLK // 2) + i * (STEP // BLOCK)
            rows = pl.ds(b * BLOCK, STEP)
            vv = jnp.concatenate(
                [
                    jnp.concatenate([v_v[slot_of(r, b + u, j)[0]] for j in range(NPB)], axis=0)
                    for u in (0, 1)
                ],
                axis=1,
            )
            o = jnp.dot(e_v[r, rows, :], vv, preferred_element_type=F32)
            part_v[r, pl.ds(b * BLOCK, BLOCK), :] = o[:BLOCK, :HD].astype(BF)
            part_v[r, pl.ds((b + 1) * BLOCK, BLOCK), :] = o[BLOCK:, HD:].astype(BF)

    def r_copy(d, m, i, src, dst):
        n = i if m == 0 else 4 + i
        return remote(src, dst, ss.at[0], rr.at[n], dev(dx=1 if d == 0 else -1))

    def r_send(d, m, i, src, dst):
        cp = r_copy(d, m, i, src, dst)
        cp.start()

    near = (1, 3)

    def far(i):
        values([(2, 0, i), (2, 1, i)])
        for d in (0, 1):
            here = pl.ds(i * STEP, STEP)
            r_send(d, 0, i, part_v.at[2, step_rows(d, i)], rly_v.at[d, here])

    def direct(i):
        values([(near[0], 1, i), (near[1], 0, i)])
        for d in (0, 1):
            rows = step_rows(1 - d, i)
            r_send(d, 1, i, part_v.at[near[d], rows], rrecv_v.at[d, rows])

    def relayed(i):
        values([(near[0], 0, i), (near[1], 1, i)])

    def own(i):
        values([(0, 0, i), (0, 1, i)])

    def relay(i):
        landed(rly_v.at[:, pl.ds(0, STEP)], rr.at[i])
        for d in (0, 1):
            rows = step_rows(d, i)
            here = pl.ds(i * STEP, STEP)
            both = rly_v[d, here, :].astype(F32) + part_v[near[d], rows, :].astype(F32)
            sum_v[d, here, :] = both.astype(BF)
            r_send(d, 2, i, sum_v.at[d, here], rrecv_v.at[d, rows])

    def y_copy(d, m, half, i, sending):
        sign = 1 if d == 0 else -1
        back = (0 if m < 2 else 1) + (0 if sending else 1)
        head = lax.rem(y - sign * back + NY, NY)
        block = att_v.at[head, step_rows(half, i)]
        n = i if m == d else 4 + i
        return remote(block, block, ss.at[0], yr.at[n], dev(dy=sign))

    def y_send(d, m, half, i):
        cp = y_copy(d, m, half, i, True)
        cp.start()

    def attend(i):
        landed(rrecv_v.at[0, pl.ds(0, 4 * STEP)], rr.at[4 + i])
        for half in (0, 1):
            rows = step_rows(half, i)
            pair = half * 4 + i
            row = tot_v[0, pair : pair + 1, :]
            for r in (1, 2, 3):
                row = row + totg_v[r, pair : pair + 1, :]
            total = jnp.sum(jnp.where(eye, row, 0.0), axis=1, keepdims=True)
            summed = (
                part_v[0, rows, :].astype(F32)
                + rrecv_v[0, rows, :].astype(F32)
                + rrecv_v[1, rows, :].astype(F32)
            )
            att_v[y, rows, :] = (summed * (1.0 / total)).astype(BF)
        for first in (0, 1):
            for d in (0, 1):
                half = d if first == 0 else 1 - d
                y_send(d, half, half, i)

    def y_forward(i):
        landed(att_v.at[0, pl.ds(0, 2 * STEP)], yr.at[i])
        for d in (0, 1):
            y_send(d, 2, d, i)

    far(0)
    far(1)
    direct(0)
    relayed(0)
    far(2)
    relay(0)
    direct(1)
    relayed(1)
    far(3)
    relay(1)
    direct(2)
    relayed(2)
    own(0)
    relay(2)
    direct(3)
    relayed(3)
    own(1)
    landed(totg_v.at[pl.ds(1, NX - 1)], tr.at[0])
    attend(0)
    relay(3)
    own(2)
    own(3)
    for load in pool_loads:
        load.wait()
    window = lax.shift_left(jnp.int32(2), y.astype(jnp.int32))
    band = jnp.where((col_id <= row_id) & (col_id > row_id - window), 1.0, 0.0).astype(BF)
    position = lax.broadcasted_iota(jnp.int32, (SEQ, GW), 0)
    inverse = 1.0 / jnp.minimum(position + 1, window).astype(F32)
    ps_all = ps_v[...].astype(F32).reshape(1, NY * GW)
    gw_all = gw_v[...].reshape(1, NY * GW)
    ps = jnp.zeros((1, GW), F32)
    gw = jnp.zeros((1, GW), F32)
    for g in range(NY):
        here = y == g
        ps = ps + jnp.where(here, ps_all[:, g * GW : (g + 1) * GW], 0.0)
        gw = gw + jnp.where(here, gw_all[:, g * GW : (g + 1) * GW], 0.0)

    def pool_step(i):
        rows = pl.ds(i * SEQ, SEQ)
        p = pooled_v[rows, :]
        pf = p.astype(F32)
        sums = jnp.dot(band, p, preferred_element_type=F32)
        residual = (sums * inverse - pf).astype(BF)
        pool_v[rows, :] = jnp.dot(residual, wm_v[...], preferred_element_type=F32) * ps
        gate_v[rows, :] = 1.0 / (1.0 + jnp.exp(-(pf * gw)))

    pool_step(0)
    pool_step(4)
    attend(1)
    pool_step(1)
    pool_step(5)
    attend(2)
    y_forward(0)
    attend(3)
    y_forward(1)
    pool_step(2)
    pool_step(6)
    y_forward(2)
    pool_step(3)
    pool_step(7)
    wc_own.wait()
    landed(wc_v.at[pl.ds(0, NY - 1)], wcr.at[0])
    wc = wc_v[...].reshape(NY * HD, GW)

    def cross(i):
        landed(att_v.at[0, pl.ds(0, 4 * STEP)], yr.at[4 + i])
        for half in (0, 1):
            rows = step_rows(half, i)
            att = jnp.concatenate([att_v[h, rows, :] for h in range(NY)], axis=1)
            term = jnp.dot(att, wc, preferred_element_type=F32)
            mixed = pool_v[rows, :] + gate_v[rows, :] * term
            out_v[rows, :] = mixed.astype(BF)

    cross(0)
    y_forward(3)
    cross(1)
    cross(2)
    cross(3)
    landed(idv.at[pl.ds(0, NX - 1)], ids_ss.at[0])
    landed(tot_v.at[pl.ds(0, NX - 1)], ts.at[0])
    landed(tok_v.at[pl.ds(0, SENT_ROWS)], ss.at[0])


def per_device(
    tokens, passage_ids, store, mix_gain, w_query, w_key, w_value, w_cross_out,
    head_scale, w_pool_in, w_pool_mix, pool_scale, gate_weight,
):
    in_hbm = pl.BlockSpec(memory_space=pltpu.HBM)
    dma = pltpu.SemaphoreType.DMA
    in_specs = [in_hbm] * 13
    in_specs[8] = pl.BlockSpec(memory_space=pltpu.SMEM)
    v = pltpu.VMEM
    return pl.pallas_call(
        kernel,
        out_shape=jax.ShapeDtypeStruct((ROWS, GW), BF),
        in_specs=in_specs,
        out_specs=pl.BlockSpec(memory_space=pltpu.VMEM),
        scratch_shapes=[
            v((ROWS, D), BF),
            v((OWN, PLEN, D), BF),
            v((D, 2 * HD), BF),
            v((D, HD + GW), BF),
            v((OWN * PLEN, 2 * HD), F32),
            v((TCHUNK, HD + GW), F32),
            v((TCHUNK, 128), F32),
            v((GW, GW), BF),
            v((D,), BF),
            v((NY * GW,), BF),
            v((NY * GW,), F32),
            v((SLOTS, HD, PLEN), BF),
            v((SLOTS, PLEN, HD), BF),
            v((NX, ROWS, HD), BF),
            v((NX, NPB, NBLK), jnp.int32),
            v((2, NX, NPB, NBLK), jnp.int32),
            pltpu.SMEM((2, NX, NPB, NBLK), jnp.int32),
            v((NY, HD, GW), BF),
            v((ROWS, GW), BF),
            v((ROWS, GW), F32),
            v((ROWS, GW), F32),
            v((NX, ROWS, NPB * PLEN), BF),
            v((NX, ROWS, HD), BF),
            v((2, ROWS // 2, HD), BF),
            v((2, ROWS // 2, HD), BF),
            v((2, ROWS, HD), BF),
            v((NX, 8, 128), F32),
            v((NX, 8, 128), F32),
            v((NY, ROWS, HD), BF),
            dma((17,)),
            dma((PIECES,)),
            dma((1,)),
            dma((23,)),
            dma((2,)),
            dma((8,)),
            dma((1,)), dma((1,)),
            dma((1,)),
            dma((1,)), dma((1,)),
            dma((8,)),
            dma((8,)),
        ],
        compiler_params=pltpu.CompilerParams(
            collective_id=0, has_side_effects=True, vmem_limit_bytes=60 * 1024 * 1024
        ),
        name="mixer",
    )(
        tokens, passage_ids.T, store, mix_gain, w_query, w_key, w_value, w_cross_out,
        head_scale, w_pool_in, w_pool_mix, pool_scale, gate_weight,
    )


def solution(mesh):
    return jax.shard_map(
        per_device,
        mesh=mesh,
        in_specs=(
            P("st", None),
            P("st", None),
            P("st", None, None),
            P(),
            P(None, "tp"),
            P(None, "tp"),
            P(None, "tp"),
            P("tp", None),
            P(),
            P(None, "tp"),
            P(),
            P(),
            P(),
        ),
        out_specs=P("st", "tp"),
        check_vma=False,
    )
```
